128 devices in a mesh: sp: 64 (over z, y, x), tp: 2 (over core).
Axes of the slice: x: 4, y: 4, z: 4, core: 2. Of those that a mesh axis runs over, the one named last changes fastest.
Arguments:
- mid_stream: bfloat16 [20480, 2048], P('sp', 'tp'), may hold values from -6 to 6
- layer_cot: bfloat16 [20480, 2048], P('sp', 'tp'), may hold values from -16 to 16
- ffn_gain: bfloat16 [2048], P('tp'), may hold values from 0.099609375 to 1.8984375
- expert_ids: int32 [20480, 2], P('sp'), may hold values from 0 to 63, all different within a row; in each aligned block of 320 rows (0 to 319, 320 to 639, ...) at most 20 rows name the same one
- group_prob: float32 [20480], P('sp'), may hold values from 0.25 to 1
- first_share: float32 [20480], P('sp'), may hold values from 0.5 to 0.95
- expert_gate: bfloat16 [64, 2048, 1024], P('sp', None, 'tp'), may hold values from -0.125 to 0.125
- expert_up: bfloat16 [64, 2048, 1024], P('sp', None, 'tp'), may hold values from -0.125 to 0.125
- expert_down: bfloat16 [64, 1024, 2048], P('sp', 'tp'), may hold values from -0.1875 to 0.1875
- out_weight: bfloat16 [2048, 1024], P(None, 'tp'), may hold values from -0.1875 to 0.1875
- conv_gain: bfloat16 [1024], P('tp'), may hold values from 0.099609375 to 1.8984375
- b_gate: bfloat16 [20480, 1024], P('sp', 'tp'), may hold values from -6 to 6
- c_gate: bfloat16 [20480, 1024], P('sp', 'tp'), may hold values from -6 to 6
- conv_in: bfloat16 [20480, 1024], P('sp', 'tp'), may hold values from -6 to 6
- conv_out: bfloat16 [20480, 1024], P('sp', 'tp'), may hold values from -6 to 6
- conv_taps: bfloat16 [3, 1024], P(None, 'tp'), may hold values from -3.5 to 3.5
Outputs:
- grad_gate: float32 [64, 2048, 1024], P('sp', None, 'tp')
- grad_up: float32 [64, 2048, 1024], P('sp', None, 'tp')
- grad_down: float32 [64, 1024, 2048], P('sp', 'tp')
- grad_out_weight: float32 [2048, 1024], P('sp', 'tp')
- mid_grad: bfloat16 [20480, 2048], P('sp', 'tp')
- grad_b: bfloat16 [20480, 1024], P('sp', 'tp')
- grad_c: bfloat16 [20480, 1024], P('sp', 'tp')
- grad_conv_in: bfloat16 [20480, 1024], P('sp', 'tp')
The draws below stay inside these ranges and needn't reach their ends.
Inputs may be any that keep to these rules, and one draw needn't show every extreme that they name: `expert_ids`: each row names 2 different experts. Among the rows of one device no expert is named more than 20 times, a bound that some block reaches.
All inputs are finite; a program needn't handle non-finite values.
Results may differ from the reference program's by a relative error of at most 0.0067.
Values may be sent and summed in bfloat16 or wider, within the bound.
A program may use at most 128 MiB of HBM per device.

```python
import math
import jax
import jax.numpy as jnp
import numpy as np
from jax import lax

D = 2048
CONV_CH = 1024
GROUP = 64
FF = 1024
TOP = 2
TOK_DEV = 320
TOKENS = 20480
EXPERTS = 64
CAP = 20
N_SP = 64
N_TP = 2


def with_spikes(entries, key, source, target, parts, factor):
    def block_of(position):
        return (jnp.arange(entries.shape[position]) // (entries.shape[position] // parts)).reshape((-1,) + (1,) * (entries.ndim - 1 - position))

    first = jax.random.permutation(key, parts)[block_of(target)]
    far = (block_of(target) + parts // 2) % parts
    return jnp.where((block_of(source) == first) | (block_of(source) == far), factor * entries, entries)


def block_scale(rng, dims, shards, least, high):
    gain, own = 1.0, jax.random.fold_in(rng, 6)
    for dim, blocks in shards:
        draws = jnp.exp(jax.random.uniform(jax.random.fold_in(own, dim), (blocks,), jnp.float32, least / len(shards), high / len(shards)))
        gain = gain * jnp.repeat(draws, dims[dim] // blocks).reshape([-1 if axis == dim else 1 for axis in range(len(dims))])
    return gain


def shared_out(stream_key, own, number, rows, number_of, top, limit, skew):
    order = jax.random.permutation(stream_key, number_of)
    crowded, ordinary = portions_of(number_of, rows * top, limit, skew, True), portions_of(number_of, rows * top, limit, skew, False)
    places = jnp.arange(number_of)

    def named(lengths, offset_by):
        used = int((lengths > 0).sum())
        fixed = max(1, used // 4)
        moved = fixed + (places - fixed + offset_by * (used - fixed)) % max(1, number_of - fixed)
        return jnp.zeros((number_of,), jnp.int32).at[order[jnp.where(places < fixed, places, moved)]].set(jnp.asarray(lengths, jnp.int32))

    lengths = jnp.where(number % 4 == 0, named(crowded, number // 4), named(ordinary, number - number // 4 - 1))
    mixed = jax.random.permutation(jax.random.fold_in(own, 3), number_of)
    source_of, taker = mixed[0:number_of // 2 * 2:2], mixed[1:number_of // 2 * 2:2]
    slack = jnp.minimum(lengths[source_of] - 1, limit - lengths[taker]) // 2
    slack = jnp.where((source_of == order[0]) | (taker == order[0]) | (lengths[taker] == 0), 0, jnp.maximum(slack, 0))
    moved = jax.random.randint(jax.random.fold_in(own, 4), (number_of // 2,), 0, 1 << 20) % (slack + 1)
    lengths = lengths.at[source_of].add(-moved).at[taker].add(moved)
    items = jnp.searchsorted(jnp.cumsum(lengths), jnp.arange(rows * top), side="right").astype(jnp.int32)
    table = items.reshape(top, rows).T
    table = table[jax.random.permutation(jax.random.fold_in(own, 1), rows)]
    offset_by = jax.random.randint(jax.random.fold_in(own, 2), (rows, 1), 0, top)
    return jnp.take_along_axis(table, (jnp.arange(top)[None, :] + offset_by) % top, axis=1)


def portions_of(amount, total, limit, skew, full):
    loads = [(1 << 20) // math.isqrt(rank ** skew) + 1 for rank in range(1, amount + 1)]
    largest = limit if full else min(limit, max(-(-total // amount), total * loads[0] // sum(loads)))
    least = 1 if total - largest >= amount - 1 else 0
    given, rest = [largest] + [least] * (amount - 1), total - largest - least * (amount - 1)
    while rest > 0:
        free = [i for i in range(1, amount) if given[i] < largest] or [i for i in range(1, amount) if given[i] < limit]
        pool, remaining = sum([loads[i] for i in free]), rest
        for i in free:
            addition = min(limit - given[i], max(1, remaining * loads[i] // pool), rest)
            given[i] = given[i] + addition
            rest = rest - addition
    return np.array(given)


def bell_draw(key, extent, width, limit, shards=(), held_as=jnp.bfloat16):
    values = width * jax.random.normal(key, extent, jnp.float32)
    if shards:
        values = values * block_scale(key, extent, shards, -0.22, 0.18)
    return jnp.clip(values, -limit, limit).astype(held_as)


def bell_draw_with(stream_key, shape, scale, reach, cuts, heavy, kind=jnp.bfloat16):
    result = scale * jax.random.normal(stream_key, shape, jnp.float32)
    if cuts:
        result = result * block_scale(stream_key, shape, cuts, -0.22, 0.18)
    return jnp.clip(with_spikes(result, jax.random.fold_in(stream_key, 3), *heavy), -reach, reach).astype(kind)


def setup_inputs(seed: int = 0) -> dict:
    key_of = jax.random.split(jax.random.key(seed), 17)
    mid_stream = bell_draw(key_of[0], (TOKENS, D), 1.0, 6.0, ((0, 64), (1, 2)))
    layer_cot = bell_draw_with(key_of[1], (TOKENS, D), 1.0, 16.0, ((0, 64), (1, 2)), (0, 1, 64, 4.0))
    ffn_gain = jnp.clip(1.0 + 0.18 * jax.random.normal(key_of[2], (D,), jnp.float32), 0.099609375, 1.8984375).astype(jnp.bfloat16)
    expert_ids_keys = jax.random.split(jax.random.fold_in(key_of[3], 1), TOKENS // TOK_DEV)
    expert_ids_turns = jax.random.permutation(jax.random.fold_in(key_of[3], 3), TOKENS // TOK_DEV)
    expert_ids = jax.vmap(lambda own, number: shared_out(jax.random.fold_in(key_of[3], 2), own, number, TOK_DEV, EXPERTS, TOP, CAP, 2))(expert_ids_keys, expert_ids_turns).reshape((TOKENS, TOP))
    group_prob = jnp.clip(0.25 + 0.75 * jax.random.uniform(key_of[4], (TOKENS,), jnp.float32) ** block_scale(key_of[4], (TOKENS,), ((0, 64),), -0.2, 0.2), 0.25, 1.0)
    first_share = jnp.clip(0.5 + 0.45 * jax.random.uniform(key_of[5], (TOKENS,), jnp.float32) ** block_scale(key_of[5], (TOKENS,), ((0, 64),), -0.2, 0.2), 0.5, 0.95)
    expert_gate = bell_draw(key_of[6], (EXPERTS, D, FF), D ** -0.5, 0.125, ((0, 64), (2, 2)))
    expert_up = bell_draw(key_of[7], (EXPERTS, D, FF), D ** -0.5, 0.125, ((0, 64), (2, 2)))
    expert_down = bell_draw(key_of[8], (EXPERTS, FF, D), FF ** -0.5, 0.1875, ((0, 64), (1, 2)))
    out_weight = bell_draw(key_of[9], (D, CONV_CH), CONV_CH ** -0.5, 0.1875, ((1, 2),))
    conv_gain = jnp.clip(1.0 + 0.18 * jax.random.normal(key_of[10], (CONV_CH,), jnp.float32), 0.099609375, 1.8984375).astype(jnp.bfloat16)
    b_gate = bell_draw(key_of[11], (TOKENS, CONV_CH), 1.0, 6.0, ((0, 64), (1, 2)))
    c_gate = bell_draw(key_of[12], (TOKENS, CONV_CH), 1.0, 6.0, ((0, 64), (1, 2)))
    conv_in = bell_draw(key_of[13], (TOKENS, CONV_CH), 1.0, 6.0, ((0, 64), (1, 2)))
    conv_out = bell_draw(key_of[14], (TOKENS, CONV_CH), 1.0, 6.0, ((0, 64), (1, 2)))
    conv_taps = bell_draw(key_of[15], (3, CONV_CH), 3 ** -0.5, 3.5, ((1, 2),))
    return dict(mid_stream=mid_stream, layer_cot=layer_cot, ffn_gain=ffn_gain, expert_ids=expert_ids, group_prob=group_prob, first_share=first_share, expert_gate=expert_gate, expert_up=expert_up, expert_down=expert_down, out_weight=out_weight, conv_gain=conv_gain, b_gate=b_gate, c_gate=c_gate, conv_in=conv_in, conv_out=conv_out, conv_taps=conv_taps)


epsilon = 1e-06

def silu_parts(pre):
    sigma = jax.nn.sigmoid(pre)
    return (pre * sigma, sigma * (1.0 + pre * (1.0 - sigma)))

def expert_backward(tokens_in, cots_in, gate_w, up_w, down_w):
    pre_gate = jnp.dot(tokens_in, gate_w, preferred_element_type=jnp.float32)
    pre_up = jnp.dot(tokens_in, up_w, preferred_element_type=jnp.float32)
    active, slope = silu_parts(pre_gate)
    hidden = (active * pre_up).astype(jnp.bfloat16)
    grad_down = jnp.dot(hidden.T, cots_in, preferred_element_type=jnp.float32)
    d_hidden = jnp.dot(cots_in, down_w.T, preferred_element_type=jnp.float32)
    d_gate = (d_hidden * pre_up * slope).astype(jnp.bfloat16)
    d_up = (d_hidden * active).astype(jnp.bfloat16)
    grad_gate = jnp.dot(tokens_in.T, d_gate, preferred_element_type=jnp.float32)
    grad_up = jnp.dot(tokens_in.T, d_up, preferred_element_type=jnp.float32)
    block_width = FF // N_TP
    summed = jnp.zeros((tokens_in.shape[0], D), jnp.float32)
    for block_number in range(N_TP):
        first_col = block_number * block_width
        last_col = first_col + block_width
        partial_term = jnp.dot(d_gate[:, first_col:last_col], gate_w[:, first_col:last_col].T, preferred_element_type=jnp.float32)
        partial_term = partial_term + jnp.dot(d_up[:, first_col:last_col], up_w[:, first_col:last_col].T, preferred_element_type=jnp.float32)
        rounded = lax.optimization_barrier(partial_term.astype(jnp.bfloat16))
        summed = summed + rounded.astype(jnp.float32)
    return (grad_gate, grad_up, grad_down, summed.astype(jnp.bfloat16))

def reference(mid_stream, layer_cot, ffn_gain, expert_ids, group_prob, first_share, expert_gate, expert_up, expert_down, out_weight, conv_gain, b_gate, c_gate, conv_in, conv_out, conv_taps):
    token_count = mid_stream.shape[0]
    mid32 = mid_stream.astype(jnp.float32)
    gain32 = ffn_gain.astype(jnp.float32)
    inv_rms = lax.rsqrt(lax.optimization_barrier(jnp.mean(mid32 * mid32, axis=1)) + epsilon)
    normed = (mid32 * inv_rms[:, None] * gain32).astype(jnp.bfloat16)
    shares = jnp.stack([group_prob * first_share, group_prob * (1.0 - first_share)], axis=1)
    weighted = (layer_cot.astype(jnp.float32)[:, None, :] * shares[:, :, None]).astype(jnp.bfloat16)
    flat_ids = expert_ids.reshape(-1).astype(jnp.int32)
    pair_count = flat_ids.shape[0]
    depth = N_SP * CAP
    onehot = (flat_ids[:, None] == jnp.arange(EXPERTS, dtype=jnp.int32)[None, :]).astype(jnp.int32)
    before = jnp.cumsum(onehot, axis=0) - onehot
    ranks = lax.optimization_barrier(jnp.sum(before * onehot, axis=1)).astype(jnp.int32)
    slot_index = (flat_ids * depth + ranks).astype(jnp.int32)
    source = jnp.full((EXPERTS * depth,), pair_count, jnp.int32)
    source = source.at[slot_index].set(jnp.arange(pair_count, dtype=jnp.int32)).reshape(EXPERTS, depth)
    normed_pad = jnp.concatenate([normed, jnp.zeros((1, D), jnp.bfloat16)], axis=0)
    weighted_pad = jnp.concatenate([weighted.reshape(pair_count, D), jnp.zeros((1, D), jnp.bfloat16)], axis=0)

    def per_expert(packed):
        rows_of, gate_w, up_w, down_w = packed
        tokens_in = normed_pad[rows_of // 2]
        cots_in = weighted_pad[rows_of]
        return expert_backward(tokens_in, cots_in, gate_w, up_w, down_w)
    grad_gate, grad_up, grad_down, back_all = lax.map(per_expert, (source, expert_gate, expert_up, expert_down))
    back_rows = back_all.reshape(EXPERTS * depth, D)[slot_index]
    d_normed = lax.optimization_barrier(jnp.sum(back_rows.astype(jnp.float32).reshape(token_count, TOP, D), axis=1))
    g_dn = gain32 * d_normed
    inner = lax.optimization_barrier(jnp.mean(mid32 * g_dn, axis=1))
    mid_total = layer_cot.astype(jnp.float32) + inv_rms[:, None] * g_dn - mid32 * (inv_rms ** 3 * inner)[:, None]
    mid_grad = mid_total.astype(jnp.bfloat16)
    b32 = b_gate.astype(jnp.float32)
    y32 = conv_out.astype(jnp.float32)
    grouped = (b32 * y32).reshape(token_count, CONV_CH // GROUP, GROUP)
    group_rms = lax.rsqrt(lax.optimization_barrier(jnp.mean(grouped * grouped, axis=-1)) + epsilon)
    cgain = conv_gain.astype(jnp.float32).reshape(CONV_CH // GROUP, GROUP)
    conv_normed = (grouped * group_rms[..., None] * cgain).reshape(token_count, CONV_CH).astype(jnp.bfloat16)
    grad_out_weight = jnp.dot(mid_grad.T, conv_normed, preferred_element_type=jnp.float32)
    d_normed_conv = jnp.dot(mid_grad, out_weight, preferred_element_type=jnp.float32).reshape(grouped.shape)
    g_dc = cgain * d_normed_conv
    group_inner = lax.optimization_barrier(jnp.mean(grouped * g_dc, axis=-1))
    d_gated = (group_rms[..., None] * g_dc - grouped * (group_rms ** 3 * group_inner)[..., None]).reshape(token_count, CONV_CH)
    grad_b = (d_gated * y32).astype(jnp.bfloat16)
    d_conv_out = d_gated * b32
    extended = jnp.concatenate([d_conv_out, jnp.zeros((2, CONV_CH), jnp.float32)], axis=0)
    taps = conv_taps.astype(jnp.float32)
    d_mixed = taps[2] * extended[:-2] + taps[1] * extended[1:-1] + taps[0] * extended[2:]
    grad_c = (d_mixed * conv_in.astype(jnp.float32)).astype(jnp.bfloat16)
    grad_conv_in = (d_mixed * c_gate.astype(jnp.float32)).astype(jnp.bfloat16)
    return (grad_gate, grad_up, grad_down, grad_out_weight, mid_grad, grad_b, grad_c, grad_conv_in)
```

```python
import functools

import jax
import jax.numpy as jnp
from jax import lax
from jax.experimental import pallas as pl
from jax.experimental.pallas import tpu as pltpu
from jax.sharding import PartitionSpec as P

D = 2048
HALF = 1024
GROUP = 64
TOK = 320
FF = 512
NDEV = 64
ROWS = 1280
CH = 256
epsilon = 1e-06

F32 = jnp.float32
BF16 = jnp.bfloat16
MESH = pl.DeviceIdType.MESH
VM = pl.BlockSpec(memory_space=pltpu.VMEM)
ANY = pl.BlockSpec(memory_space=pl.ANY)


def mm(a, b):
    return jnp.dot(a, b, preferred_element_type=F32)


def mm_nt(a, b):
    return lax.dot_general(a, b, (((1,), (1,)), ((), ())), preferred_element_type=F32)


def mm_tn(a, b):
    return lax.dot_general(a, b, (((0,), (0,)), ((), ())), preferred_element_type=F32)


def iota(shape, dim):
    return lax.broadcasted_iota(jnp.int32, shape, dim)


def ind(mask):
    return jnp.where(mask, 1.0, 0.0)


def greet(other):
    barrier = pltpu.get_barrier_semaphore()
    pl.semaphore_signal(barrier, inc=1, device_id=other, device_id_type=MESH)
    pl.semaphore_wait(barrier, 1)


def lane_slots(ids, ids_t):
    earlier = iota((TOK, TOK), 0) < iota((TOK, TOK), 1)
    out = []
    for c in range(2):
        mine = ids_t[c : c + 1, :]
        same = ind(earlier & (ids[:, 0:1] == mine)) + ind(earlier & (ids[:, 1:2] == mine))
        rank = jnp.sum(same, axis=0, keepdims=True).astype(jnp.int32)
        out.append(mine * 32 + rank)
    return out


def row_slots(ids, ids_t):
    earlier = iota((TOK, TOK), 1) < iota((TOK, TOK), 0)
    out = []
    for c in range(2):
        mine = ids[:, c : c + 1]
        same = ind(earlier & (ids_t[0:1, :] == mine)) + ind(earlier & (ids_t[1:2, :] == mine))
        rank = jnp.sum(same, axis=1, keepdims=True).astype(jnp.int32)
        out.append(mine * 32 + rank)
    return out


def prep_kernel(
    mid, cot, gain, ids, ids_t, prob, share, packed, inv_out, sq_mine, sq_other, normed, send, recv
):
    sp, tp = lax.axis_index("sp"), lax.axis_index("tp")
    other = (sp, 1 - tp)
    greet(other)
    m32 = mid[...].astype(F32)
    sq = jnp.sum(m32 * m32, axis=1, keepdims=True)
    sq_mine[...] = jnp.broadcast_to(sq, (TOK, 128))
    copy = pltpu.make_async_remote_copy(
        sq_mine, sq_other, send.at[0], recv.at[0], device_id=other, device_id_type=MESH
    )
    copy.start()
    slot0, slot1 = lane_slots(ids[...], ids_t[...])
    s0 = prob[...] * share[...]
    s1 = prob[...] * (1.0 - share[...])
    copy.wait()
    total = sq + sq_other[:, 0:1]
    inv = lax.rsqrt(total / D + epsilon)
    inv_out[...] = jnp.broadcast_to(inv, (TOK, 128))
    normed[...] = (m32 * inv * gain[...].astype(F32)).astype(BF16)

    def block(i, carry):
        e0 = i * 16
        r = iota((CH, 1), 0)
        code = (e0 + r // 16) * 32 + r % 16
        hit0 = code == slot0
        hit1 = code == slot1
        pick = ind(hit0 | hit1).astype(BF16)
        weight = jnp.sum(jnp.where(hit0, s0, 0.0) + jnp.where(hit1, s1, 0.0), axis=1, keepdims=True)
        tok = mm(pick, normed[...]).astype(BF16)
        ct = (mm(pick, cot[...]) * weight).astype(BF16)
        dst = pl.ds(e0, 16)
        packed[dst, 0:16, :] = tok[:, :512].reshape(16, 16, 512)
        packed[dst, 16:32, :] = tok[:, 512:].reshape(16, 16, 512)
        packed[dst, 32:48, :] = ct[:, :512].reshape(16, 16, 512)
        packed[dst, 48:64, :] = ct[:, 512:].reshape(16, 16, 512)
        part = (r // 4) % 4
        code = (e0 + r // 16) * 32 + 16 + r % 4
        hit0 = code == slot0
        hit1 = code == slot1
        hit = hit0 | hit1
        weight = jnp.sum(jnp.where(hit0, s0, 0.0) + jnp.where(hit1, s1, 0.0), axis=1, keepdims=True)
        acc = mm(ind(hit & (part == 0)).astype(BF16), normed[:, :512])
        acc += mm(ind(hit & (part == 1)).astype(BF16), normed[:, 512:])
        acc += mm(ind(hit & (part == 2)).astype(BF16), cot[:, :512])
        acc += mm(ind(hit & (part == 3)).astype(BF16), cot[:, 512:])
        acc = acc * jnp.where(part >= 2, weight, 1.0)
        packed[dst, 64:80, :] = acc.astype(BF16).reshape(16, 16, 512)
        return carry

    lax.fori_loop(0, 4, block, 0)


def prep(mid, cot, gain, ids, ids_t, prob, share):
    return pl.pallas_call(
        prep_kernel,
        name="prep",
        out_shape=(
            jax.ShapeDtypeStruct((NDEV, 80, 512), BF16),
            jax.ShapeDtypeStruct((TOK, 128), F32),
        ),
        in_specs=[VM] * 7,
        out_specs=(VM, VM),
        scratch_shapes=[
            pltpu.VMEM((TOK, 128), F32),
            pltpu.VMEM((TOK, 128), F32),
            pltpu.VMEM((TOK, HALF), BF16),
            pltpu.SemaphoreType.DMA((1,)),
            pltpu.SemaphoreType.DMA((1,)),
        ],
        compiler_params=pltpu.CompilerParams(
            collective_id=1, has_side_effects=True, vmem_limit_bytes=40 * 2**20
        ),
        cost_estimate=pl.CostEstimate(
            flops=6 * 10**9, bytes_accessed=7 * 10**6, transcendentals=0
        ),
    )(mid, cot, gain, ids, ids_t, prob, share)


def expert_kernel(
    rin,
    wg,
    wu,
    wd,
    ret,
    tok_out,
    cot_out,
    hid_out,
    dg_out,
    du_out,
    tok,
    cots,
    acc_g,
    acc_u,
    acc_h,
    hid,
    dg,
    du,
    mine,
    theirs,
    got,
    tsend,
    trecv,
    csend,
    crecv,
    bsend,
    brecv,
    osem,
):
    sp, tp = lax.axis_index("sp"), lax.axis_index("tp")
    other = (sp, 1 - tp)
    own_cols = pl.ds(pl.multiple_of(tp * HALF, HALF), HALF)
    oth_cols = pl.ds(pl.multiple_of((1 - tp) * HALF, HALF), HALF)
    greet(other)

    def rows_of(i):
        return pl.ds(pl.multiple_of(i * CH, CH), CH)

    def swap(buf, half, i, send, recv):
        return pltpu.make_async_remote_copy(
            buf.at[half, rows_of(i)],
            buf.at[half, rows_of(i)],
            send.at[i],
            recv.at[i],
            device_id=other,
            device_id_type=MESH,
        )

    def gather_a(i, carry):
        src = pl.ds(i * 16, 16)
        rows = rows_of(i)
        tok[tp, rows, 0:512] = rin[src, 0:16, :].reshape(CH, 512)
        tok[tp, rows, 512:1024] = rin[src, 16:32, :].reshape(CH, 512)
        cots[tp, rows, 0:512] = rin[src, 32:48, :].reshape(CH, 512)
        cots[tp, rows, 512:1024] = rin[src, 48:64, :].reshape(CH, 512)
        swap(tok, tp, i, tsend, trecv).start()
        swap(cots, tp, i, csend, crecv).start()
        return carry

    lax.fori_loop(0, 4, gather_a, 0)

    def gather_b(i, carry):
        mixed = rin[pl.ds(i * 16, 16), 64:80, :].reshape(CH, 512)
        rows = pl.ds(pl.multiple_of(1024 + i * 64, 64), 64)
        r = iota((64, CH), 0)
        c = iota((64, CH), 1)
        want = (r // 4) * 16 + r % 4
        for part, (buf, lo) in enumerate(((tok, 0), (tok, 512), (cots, 0), (cots, 512))):
            move = ind(c == want + part * 4).astype(BF16)
            buf[tp, rows, lo : lo + 512] = mm(move, mixed).astype(BF16)
        return carry

    lax.fori_loop(0, 4, gather_b, 0)
    swap(tok, tp, 4, tsend, trecv).start()
    swap(cots, tp, 4, csend, crecv).start()

    def own_part(i, carry):
        rows = rows_of(i)
        x = tok[tp, rows, :]
        y = cots[tp, rows, :]
        acc_g[rows, :] = mm(x, wg[own_cols, :])
        acc_u[rows, :] = mm(x, wu[own_cols, :])
        acc_h[rows, :] = mm_nt(y, wd[:, own_cols])
        return carry

    lax.fori_loop(0, 5, own_part, 0)
    keep = [
        pltpu.make_async_copy(tok.at[tp], tok_out.at[:, own_cols], osem.at[0]),
        pltpu.make_async_copy(cots.at[tp], cot_out.at[:, own_cols], osem.at[1]),
    ]
    for k in keep:
        k.start()

    def back_copy(i):
        return pltpu.make_async_remote_copy(
            theirs.at[rows_of(i)],
            got.at[rows_of(i)],
            bsend.at[i],
            brecv.at[i],
            device_id=other,
            device_id_type=MESH,
        )

    def rest(i, carry):
        rows = rows_of(i)
        swap(tok, 1 - tp, i, tsend, trecv).wait_recv()
        swap(cots, 1 - tp, i, csend, crecv).wait_recv()
        x = tok[1 - tp, rows, :]
        y = cots[1 - tp, rows, :]
        pre_g = acc_g[rows, :] + mm(x, wg[oth_cols, :])
        pre_u = acc_u[rows, :] + mm(x, wu[oth_cols, :])
        d_h = acc_h[rows, :] + mm_nt(y, wd[:, oth_cols])
        sigma = jax.nn.sigmoid(pre_g)
        active = pre_g * sigma
        slope = sigma * (1.0 + pre_g * (1.0 - sigma))
        hid[rows, :] = (active * pre_u).astype(BF16)
        g = (d_h * pre_u * slope).astype(BF16)
        u = (d_h * active).astype(BF16)
        dg[rows, :] = g
        du[rows, :] = u
        theirs[rows, :] = (mm_nt(g, wg[oth_cols, :]) + mm_nt(u, wu[oth_cols, :])).astype(BF16)
        back_copy(i).start()
        mine[rows, :] = (mm_nt(g, wg[own_cols, :]) + mm_nt(u, wu[own_cols, :])).astype(BF16)
        return carry

    lax.fori_loop(0, 5, rest, 0)
    keep2 = [
        pltpu.make_async_copy(tok.at[1 - tp], tok_out.at[:, oth_cols], osem.at[2]),
        pltpu.make_async_copy(cots.at[1 - tp], cot_out.at[:, oth_cols], osem.at[3]),
        pltpu.make_async_copy(hid, hid_out, osem.at[4]),
        pltpu.make_async_copy(dg, dg_out, osem.at[5]),
        pltpu.make_async_copy(du, du_out, osem.at[6]),
    ]
    for k in keep2:
        k.start()

    def total(rows):
        return (mine[rows, :].astype(F32) + got[rows, :].astype(F32)).astype(BF16)

    def finish_a(i, carry):
        back_copy(i).wait_recv()
        s = total(rows_of(i))
        src = pl.ds(i * 16, 16)
        for q in range(4):
            ret[src, q * 16 : (q + 1) * 16, :] = s[:, q * 256 : (q + 1) * 256].reshape(16, 16, 256)
        return carry

    lax.fori_loop(0, 4, finish_a, 0)
    back_copy(4).wait_recv()

    def finish_b(i, carry):
        s = total(pl.ds(pl.multiple_of(1024 + i * 64, 64), 64))
        r = iota((CH, 64), 0)
        c = iota((CH, 64), 1)
        want = (r // 16) * 4 + r % 4
        part = (r // 4) % 4
        acc = jnp.zeros((CH, 256), F32)
        for q in range(4):
            move = ind((c == want) & (part == q)).astype(BF16)
            acc += mm(move, s[:, q * 256 : (q + 1) * 256])
        ret[pl.ds(i * 16, 16), 64:80, :] = acc.astype(BF16).reshape(16, 16, 256)
        return carry

    lax.fori_loop(0, 4, finish_b, 0)

    def drain(i, carry):
        swap(tok, tp, i, tsend, trecv).wait_send()
        swap(cots, tp, i, csend, crecv).wait_send()
        back_copy(i).wait_send()
        return carry

    lax.fori_loop(0, 5, drain, 0)
    for k in keep + keep2:
        k.wait()


def expert(rin, wg, wu, wd):
    return pl.pallas_call(
        expert_kernel,
        name="expert",
        out_shape=(
            jax.ShapeDtypeStruct((NDEV, 80, 256), BF16),
            jax.ShapeDtypeStruct((ROWS, D), BF16),
            jax.ShapeDtypeStruct((ROWS, D), BF16),
            jax.ShapeDtypeStruct((ROWS, FF), BF16),
            jax.ShapeDtypeStruct((ROWS, FF), BF16),
            jax.ShapeDtypeStruct((ROWS, FF), BF16),
        ),
        in_specs=[VM] * 4,
        out_specs=(VM, ANY, ANY, ANY, ANY, ANY),
        scratch_shapes=[
            pltpu.VMEM((2, ROWS, HALF), BF16),
            pltpu.VMEM((2, ROWS, HALF), BF16),
            pltpu.VMEM((ROWS, FF), F32),
            pltpu.VMEM((ROWS, FF), F32),
            pltpu.VMEM((ROWS, FF), F32),
            pltpu.VMEM((ROWS, FF), BF16),
            pltpu.VMEM((ROWS, FF), BF16),
            pltpu.VMEM((ROWS, FF), BF16),
            pltpu.VMEM((ROWS, HALF), BF16),
            pltpu.VMEM((ROWS, HALF), BF16),
            pltpu.VMEM((ROWS, HALF), BF16),
            pltpu.SemaphoreType.DMA((5,)),
            pltpu.SemaphoreType.DMA((5,)),
            pltpu.SemaphoreType.DMA((5,)),
            pltpu.SemaphoreType.DMA((5,)),
            pltpu.SemaphoreType.DMA((5,)),
            pltpu.SemaphoreType.DMA((5,)),
            pltpu.SemaphoreType.DMA((7,)),
        ],
        compiler_params=pltpu.CompilerParams(
            collective_id=2, has_side_effects=True, vmem_limit_bytes=58 * 2**20
        ),
        cost_estimate=pl.CostEstimate(
            flops=14 * 10**9, bytes_accessed=30 * 10**6, transcendentals=655360
        ),
    )(rin, wg, wu, wd)


def tail_kernel(
    back,
    mid,
    cot,
    gain,
    ids,
    ids_t,
    inv_in,
    bg,
    co,
    cgain,
    ow,
    gow,
    mgrad,
    gb,
    dco,
    in_mine,
    in_other,
    mg,
    send,
    recv,
):
    sp, tp = lax.axis_index("sp"), lax.axis_index("tp")
    other = (sp, 1 - tp)
    own_rows = pl.ds(pl.multiple_of(tp * HALF, HALF), HALF)
    oth_rows = pl.ds(pl.multiple_of((1 - tp) * HALF, HALF), HALF)
    greet(other)
    slot0, slot1 = row_slots(ids[...], ids_t[...])
    r = iota((1, HALF), 1)
    code = (r // 16) * 32 + r % 16
    pick_a = ind((code == slot0) | (code == slot1)).astype(BF16)
    code = (r // 16) * 32 + 16 + r % 4
    hit = (code == slot0) | (code == slot1)
    part = (r // 4) % 4
    mixed = back[:, 64:80, :].reshape(HALF, 256)
    pieces = []
    for q in range(4):
        d = mm(pick_a, back[:, q * 16 : (q + 1) * 16, :].reshape(HALF, 256))
        d += mm(ind(hit & (part == q)).astype(BF16), mixed)
        pieces.append(d)
    g_dn = jnp.concatenate(pieces, axis=1) * gain[...].astype(F32)
    m32 = mid[...].astype(F32)
    inner = jnp.sum(m32 * g_dn, axis=1, keepdims=True)
    in_mine[...] = jnp.broadcast_to(inner, (TOK, 128))
    copy = pltpu.make_async_remote_copy(
        in_mine, in_other, send.at[0], recv.at[0], device_id=other, device_id_type=MESH
    )
    copy.start()
    b32 = bg[...].astype(F32)
    y32 = co[...].astype(F32)
    cg = cgain[...].astype(F32)
    gated = b32 * y32
    same = ind(iota((512, 512), 0) // GROUP == iota((512, 512), 1) // GROUP)

    def group_mean(v):
        hi = v.astype(BF16)
        rest = v - hi.astype(F32)
        md = rest.astype(BF16)
        lo = (rest - md.astype(F32)).astype(BF16)
        ones = same.astype(BF16)
        return (mm(hi, ones) + mm(md, ones) + mm(lo, ones)) / GROUP

    rms = lax.rsqrt(group_mean(gated * gated) + epsilon)
    conv_normed = (gated * rms * cg).astype(BF16)
    copy.wait()
    inv = inv_in[:, 0:1]
    mean = (inner + in_other[:, 0:1]) / D
    total = cot[...].astype(F32) + inv * g_dn - m32 * (inv * inv * inv * mean)
    mgb = total.astype(BF16)
    mgrad[...] = mgb
    mg[tp] = mgb
    swap = pltpu.make_async_remote_copy(
        mg.at[tp], mg.at[tp], send.at[1], recv.at[1], device_id=other, device_id_type=MESH
    )
    swap.start()
    gow[own_rows, :] = mm_tn(mgb, conv_normed).astype(BF16)
    d_cn = mm(mgb, ow[own_rows, :])
    swap.wait()
    mo = mg[1 - tp]
    gow[oth_rows, :] = mm_tn(mo, conv_normed).astype(BF16)
    g_dc = cg * (d_cn + mm(mo, ow[oth_rows, :]))
    gmean = group_mean(gated * g_dc)
    d_gated = rms * g_dc - gated * (rms * rms * rms * gmean)
    gb[...] = (d_gated * y32).astype(BF16)
    dco[...] = d_gated * b32


def tail(*args):
    return pl.pallas_call(
        tail_kernel,
        name="tail",
        out_shape=(
            jax.ShapeDtypeStruct((D, 512), BF16),
            jax.ShapeDtypeStruct((TOK, HALF), BF16),
            jax.ShapeDtypeStruct((TOK, 512), BF16),
            jax.ShapeDtypeStruct((TOK, 512), F32),
        ),
        in_specs=[VM] * 11,
        out_specs=(VM,) * 4,
        scratch_shapes=[
            pltpu.VMEM((TOK, 128), F32),
            pltpu.VMEM((TOK, 128), F32),
            pltpu.VMEM((2, TOK, HALF), BF16),
            pltpu.SemaphoreType.DMA((2,)),
            pltpu.SemaphoreType.DMA((2,)),
        ],
        compiler_params=pltpu.CompilerParams(
            collective_id=3, has_side_effects=True, vmem_limit_bytes=40 * 2**20
        ),
        cost_estimate=pl.CostEstimate(
            flops=5 * 10**9, bytes_accessed=12 * 10**6, transcendentals=0
        ),
    )(*args)


def from_behind(block, axis, distance):
    devices = range(lax.axis_size(axis))
    route = [(i - distance, i) for i in devices if i - distance in devices]
    return lax.ppermute(block, axis, route)


def contract_rows(left, right):
    return lax.dot_general(
        left, right, (((0,), (0,)), ((), ())), preferred_element_type=jnp.float32
    )


def shards(
    mid_stream,
    layer_cot,
    ffn_gain,
    expert_ids,
    group_prob,
    first_share,
    expert_gate,
    expert_up,
    expert_down,
    out_weight,
    conv_gain,
    b_gate,
    c_gate,
    conv_in,
    conv_out,
    conv_taps,
):
    ids_t = expert_ids.T
    gain = ffn_gain.reshape(1, HALF)
    packed, inv = prep(
        mid_stream,
        layer_cot,
        gain,
        expert_ids,
        ids_t,
        group_prob.reshape(1, TOK),
        first_share.reshape(1, TOK),
    )
    arrived = lax.all_to_all(packed, "sp", split_axis=0, concat_axis=0, tiled=True)
    ret, tok, cot, hid, dg, du = expert(arrived, expert_gate[0], expert_up[0], expert_down[0])
    back = lax.all_to_all(ret, "sp", split_axis=0, concat_axis=0, tiled=True)
    grad_gate = contract_rows(tok, dg)[None]
    grad_up = contract_rows(tok, du)[None]
    grad_down = contract_rows(hid, cot)[None]
    gow, mid_grad, grad_b, d_conv_out = tail(
        back,
        mid_stream,
        layer_cot,
        gain,
        expert_ids,
        ids_t,
        inv,
        b_gate,
        conv_out,
        conv_gain.reshape(1, 512),
        out_weight,
    )
    parts = lax.all_to_all(gow.reshape(NDEV, 32, 512), "sp", 0, 0, tiled=True)
    grad_out_weight = jnp.sum(parts.astype(jnp.float32), axis=0)
    following = from_behind(d_conv_out[:2], "sp", -1)
    extended = jnp.concatenate([d_conv_out, following], axis=0)
    taps = conv_taps.astype(jnp.float32)
    d_mixed = taps[2] * extended[:-2] + taps[1] * extended[1:-1] + taps[0] * extended[2:]
    grad_c = (d_mixed * conv_in.astype(jnp.float32)).astype(jnp.bfloat16)
    grad_conv_in = (d_mixed * c_gate.astype(jnp.float32)).astype(jnp.bfloat16)
    return (grad_gate, grad_up, grad_down, grad_out_weight, mid_grad, grad_b, grad_c, grad_conv_in)


def solution(mesh):
    placed = (
        P("sp", "tp"),
        P("sp", "tp"),
        P("tp"),
        P("sp", None),
        P("sp"),
        P("sp"),
        P("sp", None, "tp"),
        P("sp", None, "tp"),
        P("sp", "tp", None),
        P(None, "tp"),
        P("tp"),
        P("sp", "tp"),
        P("sp", "tp"),
        P("sp", "tp"),
        P("sp", "tp"),
        P(None, "tp"),
    )
    return jax.shard_map(
        shards,
        mesh=mesh,
        in_specs=placed,
        out_specs=(
            P("sp", None, "tp"),
            P("sp", None, "tp"),
            P("sp", "tp", None),
            P("sp", "tp"),
            P("sp", "tp"),
            P("sp", "tp"),
            P("sp", "tp"),
            P("sp", "tp"),
        ),
        check_vma=False,
    )
```

```python
import functools

import jax
import jax.numpy as jnp
from jax import lax
from jax.experimental import pallas as pl
from jax.experimental.pallas import tpu as pltpu
from jax.sharding import PartitionSpec as P

D = 2048
HALF = 1024
GROUP = 64
TOK = 320
FF = 512
NDEV = 64
ROWS = 1280
JOBS = 10
RING = 3
epsilon = 1e-06

F32 = jnp.float32
BF16 = jnp.bfloat16
MESH = pl.DeviceIdType.MESH
VM = pl.BlockSpec(memory_space=pltpu.VMEM)
ANY = pl.BlockSpec(memory_space=pl.ANY)


def mm(a, b):
    return jnp.dot(a, b, preferred_element_type=F32)


def mm_nt(a, b):
    return lax.dot_general(a, b, (((1,), (1,)), ((), ())), preferred_element_type=F32)


def mm_tn(a, b):
    return lax.dot_general(a, b, (((0,), (0,)), ((), ())), preferred_element_type=F32)


def iota(shape, dim):
    return lax.broadcasted_iota(jnp.int32, shape, dim)


def ind(mask):
    return jnp.where(mask, 1.0, 0.0)


def greet(other):
    barrier = pltpu.get_barrier_semaphore()
    pl.semaphore_signal(barrier, inc=1, device_id=other, device_id_type=MESH)
    pl.semaphore_wait(barrier, 1)


def lane_slots(ids, ids_t):
    earlier = iota((TOK, TOK), 0) < iota((TOK, TOK), 1)
    out = []
    for c in range(2):
        mine = ids_t[c : c + 1, :]
        same = ind(earlier & (ids[:, 0:1] == mine)) + ind(earlier & (ids[:, 1:2] == mine))
        rank = jnp.sum(same, axis=0, keepdims=True).astype(jnp.int32)
        out.append(mine * 32 + rank)
    return out


def row_slots(ids, ids_t):
    earlier = iota((TOK, TOK), 1) < iota((TOK, TOK), 0)
    out = []
    for c in range(2):
        mine = ids[:, c : c + 1]
        same = ind(earlier & (ids_t[0:1, :] == mine)) + ind(earlier & (ids_t[1:2, :] == mine))
        rank = jnp.sum(same, axis=1, keepdims=True).astype(jnp.int32)
        out.append(mine * 32 + rank)
    return out


def row_code(r, j):
    e = ((r // 2) % 4) * 16 + ((r // 8) % 4) * 4 + r // 32
    return e * 32 + 2 * j + r % 2


def moe_kernel(
    mid,
    cot,
    gain,
    ids,
    ids_t,
    prob,
    share,
    wg,
    wu,
    wd,
    dn,
    inv_out,
    tok_out,
    cot_out,
    hid_out,
    dg_out,
    du_out,
    sq_mine,
    sq_other,
    normed,
    lanes,
    subs,
    weights,
    mix,
    unmix,
    s0,
    r1,
    r2,
    r3,
    tok_o,
    cot_o,
    tok_p,
    cot_p,
    hid,
    dg,
    du,
    mine,
    theirs,
    got,
    t0,
    t1,
    t2,
    t3,
    rows_b,
    sq_sem,
    send,
    recv,
    local,
    psend,
    precv,
    osem,
):
    sp, tp = lax.axis_index("sp"), lax.axis_index("tp")
    zz, yy, xx = sp // 16, (sp // 4) % 4, sp % 4
    other = (sp, 1 - tp)
    own_cols = pl.ds(pl.multiple_of(tp * HALF, HALF), HALF)
    oth_cols = pl.ds(pl.multiple_of((1 - tp) * HALF, HALF), HALF)

    def peer(dim, off):
        if dim == 0:
            c = (xx + off) % 4
            return c, (zz * 16 + yy * 4 + c, tp)
        if dim == 1:
            c = (yy + off) % 4
            return c, (zz * 16 + c * 4 + xx, tp)
        c = (zz + off) % 4
        return c, (c * 16 + yy * 4 + xx, tp)

    barrier = pltpu.get_barrier_semaphore()
    pl.semaphore_signal(barrier, inc=1, device_id=other, device_id_type=MESH)
    for dim in range(3):
        for off in (1, 2, 3):
            pl.semaphore_signal(barrier, inc=1, device_id=peer(dim, off)[1], device_id_type=MESH)
    pl.semaphore_wait(barrier, 10)

    m32 = mid[...].astype(F32)
    sq = jnp.sum(m32 * m32, axis=1, keepdims=True)
    sq_mine[...] = jnp.broadcast_to(sq, (TOK, 128))
    copy = pltpu.make_async_remote_copy(
        sq_mine, sq_other, sq_sem.at[0], sq_sem.at[1], device_id=other, device_id_type=MESH
    )
    copy.start()
    l0, l1 = lane_slots(ids[...], ids_t[...])
    lanes[0:1, :] = l0
    lanes[1:2, :] = l1
    b0, b1 = row_slots(ids[...], ids_t[...])
    subs[0] = jnp.broadcast_to(b0, (TOK, 128))
    subs[1] = jnp.broadcast_to(b1, (TOK, 128))
    weights[0:1, :] = prob[...] * share[...]
    weights[1:2, :] = prob[...] * (1.0 - share[...])
    i = iota((256, 256), 0)
    c = iota((256, 256), 1)
    mix[...] = ind(c == ((i // 2) % 8) * 32 + (i // 16) * 2 + i % 2).astype(BF16)
    unmix[...] = ind(c == ((i // 2) % 16) * 16 + (i // 32) * 2 + i % 2).astype(BF16)
    dn[...] = jnp.zeros((TOK, HALF), F32)
    copy.wait()
    inv = lax.rsqrt((sq + sq_other[:, 0:1]) / D + epsilon)
    inv_out[...] = jnp.broadcast_to(inv, (TOK, 128))
    normed[...] = (m32 * inv * gain[...].astype(F32)).astype(BF16)

    def part_at(buf, lead, dim, k):
        if dim == 0:
            return buf.at[lead, k]
        if dim == 1:
            return buf.at[lead, :, k]
        return buf.at[lead, :, :, k]

    def hop(stage, j):
        src, src_lead, dst, axis, depth = (
            (s0, j % RING, r1, 0, 0),
            (r1, j, r2, 1, 1),
            (r2, j, r3, 2, 2),
            (t0, j % RING, t1, 2, 0),
            (t1, j, t2, 1, 1),
            (t2, j, t3, 0, 2),
        )[stage]
        me = (xx, yy, zz)[axis]
        copies = []
        for off in (2, 1, 3):
            there, device = peer(axis, off)
            copies.append(
                pltpu.make_async_remote_copy(
                    part_at(src, src_lead, depth, there),
                    dst.at[j, me],
                    send.at[stage, j % 2, off - 1],
                    recv.at[stage, j, off - 1],
                    device_id=device,
                    device_id_type=MESH,
                )
            )
        copies.append(
            pltpu.make_async_copy(
                part_at(src, src_lead, depth, me), dst.at[j, me], local.at[stage, j % 2]
            )
        )
        return copies

    def launch(stage, j):
        for cp in hop(stage, j):
            cp.start()

    def land(stage, j):
        for cp in hop(stage, j):
            cp.wait()

    def pair(kind, j):
        src, dst = (
            (tok_o.at[j % RING], tok_p.at[j]),
            (cot_o.at[j % RING], cot_p.at[j]),
            (theirs.at[j % RING], got.at[j]),
        )[kind]
        return pltpu.make_async_remote_copy(
            src,
            dst,
            psend.at[kind, j % 2],
            precv.at[kind, j],
            device_id=other,
            device_id_type=MESH,
        )

    def keep(j):
        rows = pl.ds(pl.multiple_of(j * 128, 128), 128)
        k = j % RING
        pairs = (
            (tok_o.at[k], tok_out.at[rows, own_cols]),
            (tok_p.at[j], tok_out.at[rows, oth_cols]),
            (cot_o.at[k], cot_out.at[rows, own_cols]),
            (cot_p.at[j], cot_out.at[rows, oth_cols]),
            (hid.at[k], hid_out.at[rows]),
            (dg.at[k], dg_out.at[rows]),
            (du.at[k], du_out.at[rows]),
        )
        return [pltpu.make_async_copy(a, b, osem.at[n, j % 2]) for n, (a, b) in enumerate(pairs)]

    def select(j):
        r = iota((128, 1), 0)
        code = row_code(r, j)
        hit0 = code == lanes[0:1, :]
        hit1 = code == lanes[1:2, :]
        pick = ind(hit0 | hit1).astype(BF16)
        weight = jnp.sum(
            jnp.where(hit0, weights[0:1, :], 0.0) + jnp.where(hit1, weights[1:2, :], 0.0),
            axis=1,
            keepdims=True,
        )
        a = mm(pick, normed[...]).astype(BF16)
        b = (mm(pick, cot[...]) * weight).astype(BF16)
        for n in range(4):
            rows = slice(n * 32, n * 32 + 32)
            stack = jnp.concatenate(
                [v[rows, p * 256 : (p + 1) * 256] for v in (a, b) for p in range(4)], axis=0
            )
            s0[j % RING, n] = mm(mix[...], stack).astype(BF16).reshape(4, 4, 16, 256)
        launch(0, j)

    def unpack(j):
        k = j % RING
        for n in range(4):
            rows = slice(n * 32, n * 32 + 32)
            v = mm(unmix[...], r3[j, n].reshape(256, 256)).astype(BF16)
            for p in range(4):
                cols = slice(p * 256, (p + 1) * 256)
                tok_o[k, rows, cols] = v[p * 32 : (p + 1) * 32]
                cot_o[k, rows, cols] = v[128 + p * 32 : 128 + (p + 1) * 32]
        pair(0, j).start()
        pair(1, j).start()

    def work(j):
        k = j % RING
        pair(0, j).wait()
        pair(1, j).wait()
        xo, xp = tok_o[k], tok_p[j]
        yo, yp = cot_o[k], cot_p[j]
        pre_g = mm(xo, wg[own_cols, :]) + mm(xp, wg[oth_cols, :])
        pre_u = mm(xo, wu[own_cols, :]) + mm(xp, wu[oth_cols, :])
        d_h = mm_nt(yo, wd[:, own_cols]) + mm_nt(yp, wd[:, oth_cols])
        sigma = jax.nn.sigmoid(pre_g)
        active = pre_g * sigma
        slope = sigma * (1.0 + pre_g * (1.0 - sigma))
        hid[k] = (active * pre_u).astype(BF16)
        g = (d_h * pre_u * slope).astype(BF16)
        u = (d_h * active).astype(BF16)
        dg[k] = g
        du[k] = u
        theirs[k] = (mm_nt(g, wg[oth_cols, :]) + mm_nt(u, wu[oth_cols, :])).astype(BF16)
        pair(2, j).start()
        mine[k] = (mm_nt(g, wg[own_cols, :]) + mm_nt(u, wu[own_cols, :])).astype(BF16)
        for cp in keep(j):
            cp.start()

    def give_back(j):
        k = j % RING
        pair(2, j).wait()
        s = (mine[k].astype(F32) + got[j].astype(F32)).astype(BF16)
        for n in range(4):
            rows = slice(n * 32, n * 32 + 32)
            stack = jnp.concatenate(
                [s[rows, p * 128 : (p + 1) * 128] for p in range(8)], axis=0
            )
            t0[k, n] = mm(mix[...], stack).astype(BF16).reshape(4, 4, 16, 128)
        launch(3, j)
        for cp in keep(j):
            cp.wait()

    def collect(j):
        for n in range(4):
            rows = slice(n * 32, n * 32 + 32)
            v = mm(unmix[...], t3[j, n].reshape(256, 128)).astype(BF16)
            for p in range(8):
                rows_b[rows, p * 128 : (p + 1) * 128] = v[p * 32 : (p + 1) * 32]
        code = row_code(iota((1, 128), 1), j)
        pick = ind((code == subs[0, :, 0:1]) | (code == subs[1, :, 0:1])).astype(BF16)
        dn[...] += mm(pick, rows_b[...])

    def step(t, carry):
        def at(lag, fn):
            j = t - lag
            pl.when((j >= 0) & (j < JOBS))(lambda: fn(j))

        def relay(stage):
            def fn(j):
                land(stage, j)
                launch(stage + 1, j)

            return fn

        def arrive(j):
            land(2, j)
            unpack(j)

        def finish(j):
            land(5, j)
            collect(j)

        at(0, select)
        at(1, relay(0))
        at(2, relay(1))
        at(3, arrive)
        at(5, give_back)
        at(6, relay(3))
        at(7, relay(4))
        at(4, work)
        at(8, finish)
        return carry

    lax.fori_loop(0, JOBS + 8, step, 0)


def moe(mid, cot, gain, ids, ids_t, prob, share, wg, wu, wd):
    return pl.pallas_call(
        moe_kernel,
        name="moe",
        out_shape=(
            jax.ShapeDtypeStruct((TOK, HALF), F32),
            jax.ShapeDtypeStruct((TOK, 128), F32),
            jax.ShapeDtypeStruct((ROWS, D), BF16),
            jax.ShapeDtypeStruct((ROWS, D), BF16),
            jax.ShapeDtypeStruct((ROWS, FF), BF16),
            jax.ShapeDtypeStruct((ROWS, FF), BF16),
            jax.ShapeDtypeStruct((ROWS, FF), BF16),
        ),
        in_specs=[VM] * 10,
        out_specs=(VM, VM, ANY, ANY, ANY, ANY, ANY),
        scratch_shapes=[
            pltpu.VMEM((TOK, 128), F32),
            pltpu.VMEM((TOK, 128), F32),
            pltpu.VMEM((TOK, HALF), BF16),
            pltpu.VMEM((8, TOK), jnp.int32),
            pltpu.VMEM((2, TOK, 128), jnp.int32),
            pltpu.VMEM((8, TOK), F32),
            pltpu.VMEM((256, 256), BF16),
            pltpu.VMEM((256, 256), BF16),
            pltpu.VMEM((RING, 4, 4, 4, 16, 256), BF16),
            pltpu.VMEM((JOBS, 4, 4, 4, 16, 256), BF16),
            pltpu.VMEM((JOBS, 4, 4, 4, 16, 256), BF16),
            pltpu.VMEM((JOBS, 4, 4, 4, 16, 256), BF16),
            pltpu.VMEM((RING, 128, HALF), BF16),
            pltpu.VMEM((RING, 128, HALF), BF16),
            pltpu.VMEM((JOBS, 128, HALF), BF16),
            pltpu.VMEM((JOBS, 128, HALF), BF16),
            pltpu.VMEM((RING, 128, FF), BF16),
            pltpu.VMEM((RING, 128, FF), BF16),
            pltpu.VMEM((RING, 128, FF), BF16),
            pltpu.VMEM((RING, 128, HALF), BF16),
            pltpu.VMEM((RING, 128, HALF), BF16),
            pltpu.VMEM((JOBS, 128, HALF), BF16),
            pltpu.VMEM((RING, 4, 4, 4, 16, 128), BF16),
            pltpu.VMEM((JOBS, 4, 4, 4, 16, 128), BF16),
            pltpu.VMEM((JOBS, 4, 4, 4, 16, 128), BF16),
            pltpu.VMEM((JOBS, 4, 4, 4, 16, 128), BF16),
            pltpu.VMEM((128, HALF), BF16),
            pltpu.SemaphoreType.DMA((2,)),
            pltpu.SemaphoreType.DMA((6, 2, 3)),
            pltpu.SemaphoreType.DMA((6, JOBS, 3)),
            pltpu.SemaphoreType.DMA((6, 2)),
            pltpu.SemaphoreType.DMA((3, 2)),
            pltpu.SemaphoreType.DMA((3, JOBS)),
            pltpu.SemaphoreType.DMA((7, 2)),
        ],
        compiler_params=pltpu.CompilerParams(
            collective_id=1, has_side_effects=True, vmem_limit_bytes=62 * 2**20
        ),
        cost_estimate=pl.CostEstimate(
            flops=20 * 10**9, bytes_accessed=30 * 10**6, transcendentals=655360
        ),
    )(mid, cot, gain, ids, ids_t, prob, share, wg, wu, wd)


def tail_kernel(
    dn,
    mid,
    cot,
    gain,
    inv_in,
    bg,
    co,
    cgain,
    ow,
    gow,
    mgrad,
    gb,
    dco,
    in_mine,
    in_other,
    mg,
    send,
    recv,
):
    sp, tp = lax.axis_index("sp"), lax.axis_index("tp")
    other = (sp, 1 - tp)
    own_rows = pl.ds(pl.multiple_of(tp * HALF, HALF), HALF)
    oth_rows = pl.ds(pl.multiple_of((1 - tp) * HALF, HALF), HALF)
    greet(other)
    g_dn = dn[...] * gain[...].astype(F32)
    m32 = mid[...].astype(F32)
    inner = jnp.sum(m32 * g_dn, axis=1, keepdims=True)
    in_mine[...] = jnp.broadcast_to(inner, (TOK, 128))
    copy = pltpu.make_async_remote_copy(
        in_mine, in_other, send.at[0], recv.at[0], device_id=other, device_id_type=MESH
    )
    copy.start()
    b32 = bg[...].astype(F32)
    y32 = co[...].astype(F32)
    cg = cgain[...].astype(F32)
    gated = b32 * y32
    same = ind(iota((512, 512), 0) // GROUP == iota((512, 512), 1) // GROUP)

    def group_mean(v):
        hi = v.astype(BF16)
        rest = v - hi.astype(F32)
        md = rest.astype(BF16)
        lo = (rest - md.astype(F32)).astype(BF16)
        ones = same.astype(BF16)
        return (mm(hi, ones) + mm(md, ones) + mm(lo, ones)) / GROUP

    rms = lax.rsqrt(group_mean(gated * gated) + epsilon)
    conv_normed = (gated * rms * cg).astype(BF16)
    copy.wait()
    inv = inv_in[:, 0:1]
    mean = (inner + in_other[:, 0:1]) / D
    total = cot[...].astype(F32) + inv * g_dn - m32 * (inv * inv * inv * mean)
    mgb = total.astype(BF16)
    mgrad[...] = mgb
    mg[tp] = mgb
    swap = pltpu.make_async_remote_copy(
        mg.at[tp], mg.at[tp], send.at[1], recv.at[1], device_id=other, device_id_type=MESH
    )
    swap.start()
    gow[own_rows, :] = mm_tn(mgb, conv_normed).astype(BF16)
    d_cn = mm(mgb, ow[own_rows, :])
    swap.wait()
    mo = mg[1 - tp]
    gow[oth_rows, :] = mm_tn(mo, conv_normed).astype(BF16)
    g_dc = cg * (d_cn + mm(mo, ow[oth_rows, :]))
    gmean = group_mean(gated * g_dc)
    d_gated = rms * g_dc - gated * (rms * rms * rms * gmean)
    gb[...] = (d_gated * y32).astype(BF16)
    dco[...] = d_gated * b32


def tail(*args):
    return pl.pallas_call(
        tail_kernel,
        name="tail",
        out_shape=(
            jax.ShapeDtypeStruct((D, 512), BF16),
            jax.ShapeDtypeStruct((TOK, HALF), BF16),
            jax.ShapeDtypeStruct((TOK, 512), BF16),
            jax.ShapeDtypeStruct((TOK, 512), F32),
        ),
        in_specs=[VM] * 9,
        out_specs=(VM,) * 4,
        scratch_shapes=[
            pltpu.VMEM((TOK, 128), F32),
            pltpu.VMEM((TOK, 128), F32),
            pltpu.VMEM((2, TOK, HALF), BF16),
            pltpu.SemaphoreType.DMA((2,)),
            pltpu.SemaphoreType.DMA((2,)),
        ],
        compiler_params=pltpu.CompilerParams(
            collective_id=2, has_side_effects=True, vmem_limit_bytes=40 * 2**20
        ),
        cost_estimate=pl.CostEstimate(
            flops=5 * 10**9, bytes_accessed=12 * 10**6, transcendentals=0
        ),
    )(*args)


def from_behind(block, axis, distance):
    devices = range(lax.axis_size(axis))
    route = [(i - distance, i) for i in devices if i - distance in devices]
    return lax.ppermute(block, axis, route)


def contract_rows(left, right):
    return lax.dot_general(
        left, right, (((0,), (0,)), ((), ())), preferred_element_type=jnp.float32
    )


def shards(
    mid_stream,
    layer_cot,
    ffn_gain,
    expert_ids,
    group_prob,
    first_share,
    expert_gate,
    expert_up,
    expert_down,
    out_weight,
    conv_gain,
    b_gate,
    c_gate,
    conv_in,
    conv_out,
    conv_taps,
):
    ids_t = expert_ids.T
    gain = ffn_gain.reshape(1, HALF)
    d_normed, inv, tok, cot, hid, dg, du = moe(
        mid_stream,
        layer_cot,
        gain,
        expert_ids,
        ids_t,
        group_prob.reshape(1, TOK),
        first_share.reshape(1, TOK),
        expert_gate[0],
        expert_up[0],
        expert_down[0],
    )
    grad_gate = contract_rows(tok, dg)[None]
    grad_up = contract_rows(tok, du)[None]
    grad_down = contract_rows(hid, cot)[None]
    gow, mid_grad, grad_b, d_conv_out = tail(
        d_normed,
        mid_stream,
        layer_cot,
        gain,
        inv,
        b_gate,
        conv_out,
        conv_gain.reshape(1, 512),
        out_weight,
    )
    parts = lax.all_to_all(gow.reshape(NDEV, 32, 512), "sp", 0, 0, tiled=True)
    grad_out_weight = jnp.sum(parts.astype(jnp.float32), axis=0)
    following = from_behind(d_conv_out[:2], "sp", -1)
    extended = jnp.concatenate([d_conv_out, following], axis=0)
    taps = conv_taps.astype(jnp.float32)
    d_mixed = taps[2] * extended[:-2] + taps[1] * extended[1:-1] + taps[0] * extended[2:]
    grad_c = (d_mixed * conv_in.astype(jnp.float32)).astype(jnp.bfloat16)
    grad_conv_in = (d_mixed * c_gate.astype(jnp.float32)).astype(jnp.bfloat16)
    return (grad_gate, grad_up, grad_down, grad_out_weight, mid_grad, grad_b, grad_c, grad_conv_in)


def solution(mesh):
    placed = (
        P("sp", "tp"),
        P("sp", "tp"),
        P("tp"),
        P("sp", None),
        P("sp"),
        P("sp"),
        P("sp", None, "tp"),
        P("sp", None, "tp"),
        P("sp", "tp", None),
        P(None, "tp"),
        P("tp"),
        P("sp", "tp"),
        P("sp", "tp"),
        P("sp", "tp"),
        P("sp", "tp"),
        P(None, "tp"),
    )
    return jax.shard_map(
        shards,
        mesh=mesh,
        in_specs=placed,
        out_specs=(
            P("sp", None, "tp"),
            P("sp", None, "tp"),
            P("sp", "tp", None),
            P("sp", "tp"),
            P("sp", "tp"),
            P("sp", "tp"),
            P("sp", "tp"),
            P("sp", "tp"),
        ),
        check_vma=False,
    )
```

```python
import functools

import jax
import jax.numpy as jnp
from jax import lax
from jax.experimental import pallas as pl
from jax.experimental.pallas import tpu as pltpu
from jax.sharding import PartitionSpec as P

D = 2048
HALF = 1024
GROUP = 64
TOK = 320
FF = 512
NDEV = 64
ROWS = 1280
JOBS = 10
RING = 3
epsilon = 1e-06

F32 = jnp.float32
BF16 = jnp.bfloat16
MESH = pl.DeviceIdType.MESH
VM = pl.BlockSpec(memory_space=pltpu.VMEM)
ANY = pl.BlockSpec(memory_space=pl.ANY)


def mm(a, b):
    return jnp.dot(a, b, preferred_element_type=F32)


def mm_nt(a, b):
    return lax.dot_general(a, b, (((1,), (1,)), ((), ())), preferred_element_type=F32)


def mm_tn(a, b):
    return lax.dot_general(a, b, (((0,), (0,)), ((), ())), preferred_element_type=F32)


def iota(shape, dim):
    return lax.broadcasted_iota(jnp.int32, shape, dim)


def ind(mask):
    return jnp.where(mask, 1.0, 0.0)


def greet(other):
    barrier = pltpu.get_barrier_semaphore()
    pl.semaphore_signal(barrier, inc=1, device_id=other, device_id_type=MESH)
    pl.semaphore_wait(barrier, 1)


def lane_slots(ids, ids_t):
    earlier = iota((TOK, TOK), 0) < iota((TOK, TOK), 1)
    out = []
    for c in range(2):
        mine = ids_t[c : c + 1, :]
        same = ind(earlier & (ids[:, 0:1] == mine)) + ind(earlier & (ids[:, 1:2] == mine))
        rank = jnp.sum(same, axis=0, keepdims=True).astype(jnp.int32)
        out.append(mine * 32 + rank)
    return out


def row_slots(ids, ids_t):
    earlier = iota((TOK, TOK), 1) < iota((TOK, TOK), 0)
    out = []
    for c in range(2):
        mine = ids[:, c : c + 1]
        same = ind(earlier & (ids_t[0:1, :] == mine)) + ind(earlier & (ids_t[1:2, :] == mine))
        rank = jnp.sum(same, axis=1, keepdims=True).astype(jnp.int32)
        out.append(mine * 32 + rank)
    return out


def stride_of(dim):
    return (9 * dim * dim - 3 * dim + 2) // 2


def row_code(r, j):
    a, b, c = (stride_of((j + phase) % 3) for phase in range(3))
    e = ((r // 2) % 4) * c + ((r // 8) % 4) * b + (r // 32) * a
    return e * 32 + 2 * j + r % 2


def moe_kernel(
    mid,
    cot,
    gain,
    ids_t,
    prob,
    share,
    wg_in,
    wu_in,
    wd_in,
    dn,
    inv_out,
    tok_out,
    cot_out,
    hid_out,
    dg_out,
    du_out,
    sq_mine,
    sq_other,
    normed,
    lanes,
    subs,
    weights,
    mix,
    unmix,
    s0,
    r1,
    r2,
    r3,
    tok_o,
    cot_o,
    tok_p,
    cot_p,
    hid,
    dg,
    du,
    mine,
    theirs,
    got,
    t0,
    t1,
    t2,
    t3,
    rows_b,
    wg,
    wu,
    wd,
    sq_sem,
    send,
    recv,
    local,
    psend,
    precv,
    osem,
    wsem,
):
    sp, tp = lax.axis_index("sp"), lax.axis_index("tp")
    other = (sp, 1 - tp)
    own_cols = pl.ds(pl.multiple_of(tp * HALF, HALF), HALF)
    oth_cols = pl.ds(pl.multiple_of((1 - tp) * HALF, HALF), HALF)

    def place(dim):
        return (sp // stride_of(dim)) % 4

    def peer(dim, off):
        c = (place(dim) + off) % 4
        return c, (sp + (c - place(dim)) * stride_of(dim), tp)

    barrier = pltpu.get_barrier_semaphore()
    pl.semaphore_signal(barrier, inc=1, device_id=other, device_id_type=MESH)
    for dim in range(3):
        for off in (1, 2, 3):
            pl.semaphore_signal(barrier, inc=1, device_id=peer(dim, off)[1], device_id_type=MESH)
    loads = [
        pltpu.make_async_copy(a, b, wsem.at[n])
        for n, (a, b) in enumerate(((wg_in, wg), (wu_in, wu), (wd_in, wd)))
    ]
    for cp in loads:
        cp.start()
    m32 = mid[...].astype(F32)
    sq = jnp.sum(m32 * m32, axis=1, keepdims=True)
    sq_mine[...] = jnp.broadcast_to(sq, (TOK, 128))
    eye = ind(iota((TOK, TOK), 0) == iota((TOK, TOK), 1)).astype(BF16)
    ids = mm_nt(eye, ids_t[...].astype(F32).astype(BF16)).astype(jnp.int32)
    l0, l1 = lane_slots(ids, ids_t[...])
    lanes[0:1, :] = l0
    lanes[1:2, :] = l1
    weights[0:1, :] = prob[...] * share[...]
    weights[1:2, :] = prob[...] * (1.0 - share[...])
    i = iota((256, 256), 0)
    c = iota((256, 256), 1)
    mix[...] = ind(c == ((i // 2) % 8) * 32 + (i // 16) * 2 + i % 2).astype(BF16)
    dn[...] = jnp.zeros((TOK, HALF), F32)
    pl.semaphore_wait(barrier, 10)
    copy = pltpu.make_async_remote_copy(
        sq_mine, sq_other, sq_sem.at[0], sq_sem.at[1], device_id=other, device_id_type=MESH
    )
    copy.start()
    b0, b1 = row_slots(ids, ids_t[...])
    subs[0] = jnp.broadcast_to(b0, (TOK, 128))
    subs[1] = jnp.broadcast_to(b1, (TOK, 128))
    unmix[...] = ind(c == ((i // 2) % 16) * 16 + (i // 32) * 2 + i % 2).astype(BF16)
    copy.wait()
    inv = lax.rsqrt((sq + sq_other[:, 0:1]) / D + epsilon)
    inv_out[...] = jnp.broadcast_to(inv, (TOK, 128))
    normed[...] = (m32 * inv * gain[...].astype(F32)).astype(BF16)

    def part_at(buf, lead, depth, k):
        if depth == 0:
            return buf.at[lead, k]
        if depth == 1:
            return buf.at[lead, :, k]
        return buf.at[lead, :, :, k]

    def hop(stage, j):
        src, lead, dst = (
            (s0, j % 6, r1),
            (r1, j, r2),
            (r2, j, r3),
            (t0, (j + 2) % RING, t1),
            (t1, j, t2),
            (t2, j, t3),
        )[stage]
        dim = (j + (0, 1, 2, 2, 1, 0)[stage]) % 3
        depth = stage % 3
        me = place(dim)
        copies = []
        for off in (2, 1, 3):
            there, device = peer(dim, off)
            copies.append(
                pltpu.make_async_remote_copy(
                    part_at(src, lead, depth, there),
                    dst.at[j, me],
                    send.at[stage, j % 6, off - 1],
                    recv.at[stage, j, off - 1],
                    device_id=device,
                    device_id_type=MESH,
                )
            )
        copies.append(
            pltpu.make_async_copy(
                part_at(src, lead, depth, me), dst.at[j, me], local.at[stage, j % 6]
            )
        )
        return copies

    def launch(stage, j):
        for cp in hop(stage, j):
            cp.start()

    def land(stage, j):
        for cp in hop(stage, j):
            cp.wait()

    def pair(kind, j):
        src, dst = (
            (tok_o.at[(j + 2) % RING], tok_p.at[j]),
            (cot_o.at[(j + 2) % RING], cot_p.at[j]),
            (theirs.at[(j + 2) % RING], got.at[j]),
        )[kind]
        return pltpu.make_async_remote_copy(
            src,
            dst,
            psend.at[kind, j % RING],
            precv.at[kind, j],
            device_id=other,
            device_id_type=MESH,
        )

    def keep(j):
        rows = pl.ds(pl.multiple_of(j * 128, 128), 128)
        k = (j + 2) % RING
        pairs = (
            (tok_o.at[k], tok_out.at[rows, own_cols]),
            (tok_p.at[j], tok_out.at[rows, oth_cols]),
            (cot_o.at[k], cot_out.at[rows, own_cols]),
            (cot_p.at[j], cot_out.at[rows, oth_cols]),
            (hid.at[k], hid_out.at[rows]),
            (dg.at[k], dg_out.at[rows]),
            (du.at[k], du_out.at[rows]),
        )
        return [pltpu.make_async_copy(a, b, osem.at[n, j % RING]) for n, (a, b) in enumerate(pairs)]

    def select(j):
        r = iota((128, 1), 0)
        code = row_code(r, j)
        hit0 = code == lanes[0:1, :]
        hit1 = code == lanes[1:2, :]
        pick = ind(hit0 | hit1).astype(BF16)
        weight = jnp.sum(
            jnp.where(hit0, weights[0:1, :], 0.0) + jnp.where(hit1, weights[1:2, :], 0.0),
            axis=1,
            keepdims=True,
        )
        a = mm(pick, normed[...]).astype(BF16)
        b = (mm(pick, cot[...]) * weight).astype(BF16)
        for n in range(4):
            rows = slice(n * 32, n * 32 + 32)
            stack = jnp.concatenate(
                [v[rows, p * 256 : (p + 1) * 256] for v in (a, b) for p in range(4)], axis=0
            )
            s0[j % 6, n] = mm(mix[...], stack).astype(BF16).reshape(4, 4, 16, 256)
        launch(0, j)

    def settle(j):
        for cp in keep(j):
            cp.wait()

    def unpack(j):
        k = (j + 2) % RING
        pl.when(j >= RING)(lambda: settle(j - RING))
        for n in range(4):
            rows = slice(n * 32, n * 32 + 32)
            v = mm(unmix[...], r3[j, n].reshape(256, 256)).astype(BF16)
            for p in range(4):
                cols = slice(p * 256, (p + 1) * 256)
                tok_o[k, rows, cols] = v[p * 32 : (p + 1) * 32]
                cot_o[k, rows, cols] = v[128 + p * 32 : 128 + (p + 1) * 32]
        pair(0, j).start()
        pair(1, j).start()

    def work(j0, n):
        m = n * 128
        ring = pl.ds(2 if n == 1 else 0, n)
        jobs = pl.ds(j0, n)
        xo, yo = tok_o[ring].reshape(m, HALF), cot_o[ring].reshape(m, HALF)
        pre_g = mm(xo, wg[own_cols, :])
        pre_u = mm(xo, wu[own_cols, :])
        d_h = mm_nt(yo, wd[:, own_cols])
        for d in range(n):
            pair(0, j0 + d).wait()
            pair(1, j0 + d).wait()
        xp, yp = tok_p[jobs].reshape(m, HALF), cot_p[jobs].reshape(m, HALF)
        pre_g += mm(xp, wg[oth_cols, :])
        pre_u += mm(xp, wu[oth_cols, :])
        d_h += mm_nt(yp, wd[:, oth_cols])
        sigma = jax.nn.sigmoid(pre_g)
        active = pre_g * sigma
        slope = sigma * (1.0 + pre_g * (1.0 - sigma))
        hid[ring] = (active * pre_u).astype(BF16).reshape(n, 128, FF)
        g = (d_h * pre_u * slope).astype(BF16)
        u = (d_h * active).astype(BF16)
        dg[ring] = g.reshape(n, 128, FF)
        du[ring] = u.reshape(n, 128, FF)
        back = mm_nt(g, wg[oth_cols, :]) + mm_nt(u, wu[oth_cols, :])
        theirs[ring] = back.astype(BF16).reshape(n, 128, HALF)
        for d in range(n):
            pair(2, j0 + d).start()
        back = mm_nt(g, wg[own_cols, :]) + mm_nt(u, wu[own_cols, :])
        mine[ring] = back.astype(BF16).reshape(n, 128, HALF)
        for d in range(n):
            for cp in keep(j0 + d):
                cp.start()

    def give_back(j):
        k = (j + 2) % RING
        pair(2, j).wait()
        s = (mine[k].astype(F32) + got[j].astype(F32)).astype(BF16)
        for n in range(4):
            rows = slice(n * 32, n * 32 + 32)
            stack = jnp.concatenate(
                [s[rows, p * 128 : (p + 1) * 128] for p in range(8)], axis=0
            )
            t0[k, n] = mm(mix[...], stack).astype(BF16).reshape(4, 4, 16, 128)
        launch(3, j)

    def collect(j):
        for n in range(4):
            rows = slice(n * 32, n * 32 + 32)
            v = mm(unmix[...], t3[j, n].reshape(256, 128)).astype(BF16)
            for p in range(8):
                rows_b[rows, p * 128 : (p + 1) * 128] = v[p * 32 : (p + 1) * 32]
        code = row_code(iota((1, 128), 1), j)
        pick = ind((code == subs[0, :, 0:1]) | (code == subs[1, :, 0:1])).astype(BF16)
        dn[...] += mm(pick, rows_b[...])

    def relay(stage):
        def fn(j):
            land(stage, j)
            launch(stage + 1, j)

        return fn

    def arrive(j):
        land(2, j)
        unpack(j)

    def finish(j):
        land(5, j)
        collect(j)

    def trio(group, fn):
        def one(c, carry):
            j = group * 3 - 2 + c
            pl.when((j >= 0) & (j < JOBS))(lambda: fn(j))
            return carry

        lax.fori_loop(0, 3, one, 0)

    def step(t, carry):
        trio(t - 5, relay(4))
        trio(t - 4, relay(3))
        trio(t - 2, relay(1))
        trio(t - 1, relay(0))
        trio(t + 1, select)
        trio(t - 3, arrive)
        pl.when(t == 3)(lambda: work(0, 1))
        pl.when((t > 3) & (t < 7))(lambda: work(3 * t - 11, 3))
        trio(t - 6, finish)
        trio(t - 3, give_back)
        return carry

    select(0)
    trio(1, select)
    for cp in loads:
        cp.wait()
    lax.fori_loop(1, 10, step, 0)
    for j in range(JOBS - RING, JOBS):
        settle(j)


def moe(mid, cot, gain, ids_t, prob, share, wg, wu, wd):
    return pl.pallas_call(
        moe_kernel,
        name="moe",
        out_shape=(
            jax.ShapeDtypeStruct((TOK, HALF), F32),
            jax.ShapeDtypeStruct((TOK, 128), F32),
            jax.ShapeDtypeStruct((ROWS, D), BF16),
            jax.ShapeDtypeStruct((ROWS, D), BF16),
            jax.ShapeDtypeStruct((ROWS, FF), BF16),
            jax.ShapeDtypeStruct((ROWS, FF), BF16),
            jax.ShapeDtypeStruct((ROWS, FF), BF16),
        ),
        in_specs=[VM] * 6 + [ANY] * 3,
        out_specs=(VM, VM, ANY, ANY, ANY, ANY, ANY),
        scratch_shapes=[
            pltpu.VMEM((TOK, 128), F32),
            pltpu.VMEM((TOK, 128), F32),
            pltpu.VMEM((TOK, HALF), BF16),
            pltpu.VMEM((8, TOK), jnp.int32),
            pltpu.VMEM((2, TOK, 128), jnp.int32),
            pltpu.VMEM((8, TOK), F32),
            pltpu.VMEM((256, 256), BF16),
            pltpu.VMEM((256, 256), BF16),
            pltpu.VMEM((6, 4, 4, 4, 16, 256), BF16),
            pltpu.VMEM((JOBS, 4, 4, 4, 16, 256), BF16),
            pltpu.VMEM((JOBS, 4, 4, 4, 16, 256), BF16),
            pltpu.VMEM((JOBS, 4, 4, 4, 16, 256), BF16),
            pltpu.VMEM((RING, 128, HALF), BF16),
            pltpu.VMEM((RING, 128, HALF), BF16),
            pltpu.VMEM((JOBS, 128, HALF), BF16),
            pltpu.VMEM((JOBS, 128, HALF), BF16),
            pltpu.VMEM((RING, 128, FF), BF16),
            pltpu.VMEM((RING, 128, FF), BF16),
            pltpu.VMEM((RING, 128, FF), BF16),
            pltpu.VMEM((RING, 128, HALF), BF16),
            pltpu.VMEM((RING, 128, HALF), BF16),
            pltpu.VMEM((JOBS, 128, HALF), BF16),
            pltpu.VMEM((RING, 4, 4, 4, 16, 128), BF16),
            pltpu.VMEM((JOBS, 4, 4, 4, 16, 128), BF16),
            pltpu.VMEM((JOBS, 4, 4, 4, 16, 128), BF16),
            pltpu.VMEM((JOBS, 4, 4, 4, 16, 128), BF16),
            pltpu.VMEM((128, HALF), BF16),
            pltpu.VMEM((D, FF), BF16),
            pltpu.VMEM((D, FF), BF16),
            pltpu.VMEM((FF, D), BF16),
            pltpu.SemaphoreType.DMA((2,)),
            pltpu.SemaphoreType.DMA((6, 6, 3)),
            pltpu.SemaphoreType.DMA((6, JOBS, 3)),
            pltpu.SemaphoreType.DMA((6, 6)),
            pltpu.SemaphoreType.DMA((3, RING)),
            pltpu.SemaphoreType.DMA((3, JOBS)),
            pltpu.SemaphoreType.DMA((7, RING)),
            pltpu.SemaphoreType.DMA((3,)),
        ],
        compiler_params=pltpu.CompilerParams(
            collective_id=1, has_side_effects=True, vmem_limit_bytes=62 * 2**20
        ),
        cost_estimate=pl.CostEstimate(
            flops=20 * 10**9, bytes_accessed=30 * 10**6, transcendentals=655360
        ),
    )(mid, cot, gain, ids_t, prob, share, wg, wu, wd)


def tail_kernel(
    dn,
    mid,
    cot,
    gain,
    inv_in,
    bg,
    co,
    cgain,
    ow,
    gow,
    mgrad,
    gb,
    dco,
    in_mine,
    in_other,
    mg,
    send,
    recv,
):
    sp, tp = lax.axis_index("sp"), lax.axis_index("tp")
    other = (sp, 1 - tp)
    own_rows = pl.ds(pl.multiple_of(tp * HALF, HALF), HALF)
    oth_rows = pl.ds(pl.multiple_of((1 - tp) * HALF, HALF), HALF)
    greet(other)
    g_dn = dn[...] * gain[...].astype(F32)
    m32 = mid[...].astype(F32)
    inner = jnp.sum(m32 * g_dn, axis=1, keepdims=True)
    in_mine[...] = jnp.broadcast_to(inner, (TOK, 128))
    copy = pltpu.make_async_remote_copy(
        in_mine, in_other, send.at[0], recv.at[0], device_id=other, device_id_type=MESH
    )
    copy.start()
    b32 = bg[...].astype(F32)
    y32 = co[...].astype(F32)
    cg = cgain[...].astype(F32)
    gated = b32 * y32
    same = ind(iota((512, 512), 0) // GROUP == iota((512, 512), 1) // GROUP)

    def group_mean(v):
        hi = v.astype(BF16)
        rest = v - hi.astype(F32)
        md = rest.astype(BF16)
        lo = (rest - md.astype(F32)).astype(BF16)
        ones = same.astype(BF16)
        return (mm(hi, ones) + mm(md, ones) + mm(lo, ones)) / GROUP

    rms = lax.rsqrt(group_mean(gated * gated) + epsilon)
    conv_normed = (gated * rms * cg).astype(BF16)
    copy.wait()
    inv = inv_in[:, 0:1]
    mean = (inner + in_other[:, 0:1]) / D
    total = cot[...].astype(F32) + inv * g_dn - m32 * (inv * inv * inv * mean)
    mgb = total.astype(BF16)
    mgrad[...] = mgb
    mg[tp] = mgb
    swap = pltpu.make_async_remote_copy(
        mg.at[tp], mg.at[tp], send.at[1], recv.at[1], device_id=other, device_id_type=MESH
    )
    swap.start()
    gow[own_rows, :] = mm_tn(mgb, conv_normed).astype(BF16)
    d_cn = mm(mgb, ow[own_rows, :])
    swap.wait()
    mo = mg[1 - tp]
    gow[oth_rows, :] = mm_tn(mo, conv_normed).astype(BF16)
    g_dc = cg * (d_cn + mm(mo, ow[oth_rows, :]))
    gmean = group_mean(gated * g_dc)
    d_gated = rms * g_dc - gated * (rms * rms * rms * gmean)
    gb[...] = (d_gated * y32).astype(BF16)
    dco[...] = d_gated * b32


def tail(*args):
    return pl.pallas_call(
        tail_kernel,
        name="tail",
        out_shape=(
            jax.ShapeDtypeStruct((D, 512), BF16),
            jax.ShapeDtypeStruct((TOK, HALF), BF16),
            jax.ShapeDtypeStruct((TOK, 512), BF16),
            jax.ShapeDtypeStruct((TOK, 512), F32),
        ),
        in_specs=[VM] * 9,
        out_specs=(VM,) * 4,
        scratch_shapes=[
            pltpu.VMEM((TOK, 128), F32),
            pltpu.VMEM((TOK, 128), F32),
            pltpu.VMEM((2, TOK, HALF), BF16),
            pltpu.SemaphoreType.DMA((2,)),
            pltpu.SemaphoreType.DMA((2,)),
        ],
        compiler_params=pltpu.CompilerParams(
            collective_id=2, has_side_effects=True, vmem_limit_bytes=40 * 2**20
        ),
        cost_estimate=pl.CostEstimate(
            flops=5 * 10**9, bytes_accessed=12 * 10**6, transcendentals=0
        ),
    )(*args)


def from_behind(block, axis, distance):
    devices = range(lax.axis_size(axis))
    route = [(i - distance, i) for i in devices if i - distance in devices]
    return lax.ppermute(block, axis, route)


def contract_rows(left, right):
    return lax.dot_general(
        left, right, (((0,), (0,)), ((), ())), preferred_element_type=jnp.float32
    )


def shards(
    mid_stream,
    layer_cot,
    ffn_gain,
    expert_ids,
    group_prob,
    first_share,
    expert_gate,
    expert_up,
    expert_down,
    out_weight,
    conv_gain,
    b_gate,
    c_gate,
    conv_in,
    conv_out,
    conv_taps,
):
    gain = ffn_gain.reshape(1, HALF)
    d_normed, inv, tok, cot, hid, dg, du = moe(
        mid_stream,
        layer_cot,
        gain,
        expert_ids.T,
        group_prob.reshape(1, TOK),
        first_share.reshape(1, TOK),
        expert_gate[0],
        expert_up[0],
        expert_down[0],
    )
    grad_gate = contract_rows(tok, dg)[None]
    grad_up = contract_rows(tok, du)[None]
    grad_down = contract_rows(hid, cot)[None]
    gow, mid_grad, grad_b, d_conv_out = tail(
        d_normed,
        mid_stream,
        layer_cot,
        gain,
        inv,
        b_gate,
        conv_out,
        conv_gain.reshape(1, 512),
        out_weight,
    )
    parts = lax.all_to_all(gow.reshape(NDEV, 32, 512), "sp", 0, 0, tiled=True)
    grad_out_weight = jnp.sum(parts.astype(jnp.float32), axis=0)
    following = from_behind(d_conv_out[:2], "sp", -1)
    extended = jnp.concatenate([d_conv_out, following], axis=0)
    taps = conv_taps.astype(jnp.float32)
    d_mixed = taps[2] * extended[:-2] + taps[1] * extended[1:-1] + taps[0] * extended[2:]
    grad_c = (d_mixed * conv_in.astype(jnp.float32)).astype(jnp.bfloat16)
    grad_conv_in = (d_mixed * c_gate.astype(jnp.float32)).astype(jnp.bfloat16)
    return (grad_gate, grad_up, grad_down, grad_out_weight, mid_grad, grad_b, grad_c, grad_conv_in)


def solution(mesh):
    placed = (
        P("sp", "tp"),
        P("sp", "tp"),
        P("tp"),
        P("sp", None),
        P("sp"),
        P("sp"),
        P("sp", None, "tp"),
        P("sp", None, "tp"),
        P("sp", "tp", None),
        P(None, "tp"),
        P("tp"),
        P("sp", "tp"),
        P("sp", "tp"),
        P("sp", "tp"),
        P("sp", "tp"),
        P(None, "tp"),
    )
    return jax.shard_map(
        shards,
        mesh=mesh,
        in_specs=placed,
        out_specs=(
            P("sp", None, "tp"),
            P("sp", None, "tp"),
            P("sp", "tp", None),
            P("sp", "tp"),
            P("sp", "tp"),
            P("sp", "tp"),
            P("sp", "tp"),
            P("sp", "tp"),
        ),
        check_vma=False,
    )
```

```python
import functools

import jax
import jax.numpy as jnp
from jax import lax
from jax.experimental import pallas as pl
from jax.experimental.pallas import tpu as pltpu
from jax.sharding import PartitionSpec as P

D = 2048
HALF = 1024
GROUP = 64
TOK = 320
FF = 512
NDEV = 64
ROWS = 1280
JOBS = 10
RING = 3
epsilon = 1e-06

F32 = jnp.float32
BF16 = jnp.bfloat16
MESH = pl.DeviceIdType.MESH
VM = pl.BlockSpec(memory_space=pltpu.VMEM)
ANY = pl.BlockSpec(memory_space=pl.ANY)


def mm(a, b):
    return jnp.dot(a, b, preferred_element_type=F32)


def mm_nt(a, b):
    return lax.dot_general(a, b, (((1,), (1,)), ((), ())), preferred_element_type=F32)


def mm_tn(a, b):
    return lax.dot_general(a, b, (((0,), (0,)), ((), ())), preferred_element_type=F32)


def iota(shape, dim):
    return lax.broadcasted_iota(jnp.int32, shape, dim)


def ind(mask):
    return jnp.where(mask, 1.0, 0.0)


def greet(other):
    barrier = pltpu.get_barrier_semaphore()
    pl.semaphore_signal(barrier, inc=1, device_id=other, device_id_type=MESH)
    pl.semaphore_wait(barrier, 1)


def lane_slots(ids, ids_t):
    earlier = iota((TOK, TOK), 0) < iota((TOK, TOK), 1)
    out = []
    for c in range(2):
        mine = ids_t[c : c + 1, :]
        same = ind(earlier & (ids[:, 0:1] == mine)) + ind(earlier & (ids[:, 1:2] == mine))
        rank = jnp.sum(same, axis=0, keepdims=True).astype(jnp.int32)
        out.append(mine * 32 + rank)
    return out


def row_slots(ids, ids_t):
    earlier = iota((TOK, TOK), 1) < iota((TOK, TOK), 0)
    out = []
    for c in range(2):
        mine = ids[:, c : c + 1]
        same = ind(earlier & (ids_t[0:1, :] == mine)) + ind(earlier & (ids_t[1:2, :] == mine))
        rank = jnp.sum(same, axis=1, keepdims=True).astype(jnp.int32)
        out.append(mine * 32 + rank)
    return out


def stride_of(dim):
    return (9 * dim * dim - 3 * dim + 2) // 2


def row_code(r, j):
    a, b, c = (stride_of((j + phase) % 3) for phase in range(3))
    e = ((r // 2) % 4) * c + ((r // 8) % 4) * b + (r // 32) * a
    return e * 32 + 2 * j + r % 2


def moe_kernel(
    mid,
    cot,
    gain,
    ids_t,
    prob,
    share,
    wg_in,
    wu_in,
    wd_in,
    dn,
    inv_out,
    tok_out,
    cot_out,
    hid_out,
    dg_out,
    du_out,
    sq_mine,
    sq_other,
    normed,
    lanes,
    subs,
    weights,
    mix,
    unmix,
    s0,
    r1,
    r2,
    r3,
    tok_o,
    cot_o,
    tok_p,
    cot_p,
    hid,
    dg,
    du,
    mine,
    theirs,
    got,
    t0,
    t1,
    t2,
    t3,
    rows_b,
    wg,
    wu,
    wd,
    sq_sem,
    send,
    recv,
    local,
    psend,
    precv,
    osem,
    wsem,
):
    sp, tp = lax.axis_index("sp"), lax.axis_index("tp")
    other = (sp, 1 - tp)
    own_cols = pl.ds(pl.multiple_of(tp * HALF, HALF), HALF)
    oth_cols = pl.ds(pl.multiple_of((1 - tp) * HALF, HALF), HALF)

    def place(dim):
        return (sp // stride_of(dim)) % 4

    def peer(dim, off):
        c = (place(dim) + off) % 4
        return c, (sp + (c - place(dim)) * stride_of(dim), tp)

    barrier = pltpu.get_barrier_semaphore()
    pl.semaphore_signal(barrier, inc=1, device_id=other, device_id_type=MESH)
    for dim in range(3):
        for off in (1, 2, 3):
            pl.semaphore_signal(barrier, inc=1, device_id=peer(dim, off)[1], device_id_type=MESH)
    loads = [
        pltpu.make_async_copy(a, b, wsem.at[n])
        for n, (a, b) in enumerate(((wg_in, wg), (wu_in, wu), (wd_in, wd)))
    ]
    for cp in loads:
        cp.start()
    m32 = mid[...].astype(F32)
    sq = jnp.sum(m32 * m32, axis=1, keepdims=True)
    sq_mine[...] = jnp.broadcast_to(sq, (TOK, 128))
    eye = ind(iota((TOK, TOK), 0) == iota((TOK, TOK), 1)).astype(BF16)
    ids = mm_nt(eye, ids_t[...].astype(F32).astype(BF16)).astype(jnp.int32)
    l0, l1 = lane_slots(ids, ids_t[...])
    lanes[0:1, :] = l0
    lanes[1:2, :] = l1
    p1 = prob[...].reshape(1, TOK)
    f1 = share[...].reshape(1, TOK)
    weights[0:1, :] = p1 * f1
    weights[1:2, :] = p1 * (1.0 - f1)
    i = iota((256, 256), 0)
    c = iota((256, 256), 1)
    mix[...] = ind(c == ((i // 2) % 8) * 32 + (i // 16) * 2 + i % 2).astype(BF16)
    dn[...] = jnp.zeros((TOK, HALF), F32)
    pl.semaphore_wait(barrier, 10)
    copy = pltpu.make_async_remote_copy(
        sq_mine, sq_other, sq_sem.at[0], sq_sem.at[1], device_id=other, device_id_type=MESH
    )
    copy.start()
    b0, b1 = row_slots(ids, ids_t[...])
    subs[0] = jnp.broadcast_to(b0, (TOK, 128))
    subs[1] = jnp.broadcast_to(b1, (TOK, 128))
    unmix[...] = ind(c == ((i // 2) % 16) * 16 + (i // 32) * 2 + i % 2).astype(BF16)
    copy.wait()
    inv = lax.rsqrt((sq + sq_other[:, 0:1]) / D + epsilon)
    inv_out[...] = jnp.broadcast_to(inv, (TOK, 128))
    normed[...] = (m32 * inv * gain[...].astype(F32).reshape(1, HALF)).astype(BF16)

    def part_at(buf, lead, depth, k):
        if depth == 0:
            return buf.at[lead, k]
        if depth == 1:
            return buf.at[lead, :, k]
        return buf.at[lead, :, :, k]

    def hop(stage, j):
        src, lead, dst = (
            (s0, j, r1),
            (r1, j, r2),
            (r2, j, r3),
            (t0, (j + 2) % RING, t1),
            (t1, j, t2),
            (t2, j, t3),
        )[stage]
        dim = (j + (0, 1, 2, 2, 1, 0)[stage]) % 3
        depth = stage % 3
        me = place(dim)
        copies = []
        for off in (2, 1, 3):
            there, device = peer(dim, off)
            copies.append(
                pltpu.make_async_remote_copy(
                    part_at(src, lead, depth, there),
                    dst.at[j, me],
                    send.at[stage, j, off - 1],
                    recv.at[stage, j, off - 1],
                    device_id=device,
                    device_id_type=MESH,
                )
            )
        copies.append(
            pltpu.make_async_copy(
                part_at(src, lead, depth, me), dst.at[j, me], local.at[stage, j]
            )
        )
        return copies

    def launch(stage, j):
        for cp in hop(stage, j):
            cp.start()

    def land(stage, j):
        for cp in hop(stage, j):
            cp.wait()

    def pair(kind, j):
        src, dst = (
            (tok_o.at[(j + 2) % 6], tok_p.at[j]),
            (cot_o.at[(j + 2) % 6], cot_p.at[j]),
            (theirs.at[(j + 2) % RING], got.at[j]),
        )[kind]
        return pltpu.make_async_remote_copy(
            src,
            dst,
            psend.at[kind, j % RING],
            precv.at[kind, j],
            device_id=other,
            device_id_type=MESH,
        )

    def keep(j):
        rows = pl.ds(pl.multiple_of(j * 128, 128), 128)
        k = (j + 2) % RING
        pairs = (
            (tok_o.at[(j + 2) % 6], tok_out.at[rows, own_cols]),
            (tok_p.at[j], tok_out.at[rows, oth_cols]),
            (cot_o.at[(j + 2) % 6], cot_out.at[rows, own_cols]),
            (cot_p.at[j], cot_out.at[rows, oth_cols]),
            (hid.at[k], hid_out.at[rows]),
            (dg.at[k], dg_out.at[rows]),
            (du.at[k], du_out.at[rows]),
        )
        return [pltpu.make_async_copy(a, b, osem.at[n, j % RING]) for n, (a, b) in enumerate(pairs)]

    def select(j):
        r = iota((128, 1), 0)
        code = row_code(r, j)
        hit0 = code == lanes[0:1, :]
        hit1 = code == lanes[1:2, :]
        pick = ind(hit0 | hit1).astype(BF16)
        weight = jnp.sum(
            jnp.where(hit0, weights[0:1, :], 0.0) + jnp.where(hit1, weights[1:2, :], 0.0),
            axis=1,
            keepdims=True,
        )
        a = mm(pick, normed[...]).astype(BF16)
        b = (mm(pick, cot[...]) * weight).astype(BF16)
        for n in range(4):
            rows = slice(n * 32, n * 32 + 32)
            stack = jnp.concatenate(
                [v[rows, p * 256 : (p + 1) * 256] for v in (a, b) for p in range(4)], axis=0
            )
            s0[j, n] = mm(mix[...], stack).astype(BF16).reshape(4, 4, 16, 256)
        launch(0, j)

    def settle(j):
        for cp in keep(j):
            cp.wait()

    def unpack(j):
        k = (j + 2) % 6
        for n in range(4):
            rows = slice(n * 32, n * 32 + 32)
            v = mm(unmix[...], r3[j, n].reshape(256, 256)).astype(BF16)
            for p in range(4):
                cols = slice(p * 256, (p + 1) * 256)
                tok_o[k, rows, cols] = v[p * 32 : (p + 1) * 32]
                cot_o[k, rows, cols] = v[128 + p * 32 : 128 + (p + 1) * 32]
        pair(0, j).start()
        pair(1, j).start()

    def work(j0, n, held):
        m = n * 128
        ring = pl.ds(2 if n == 1 else 0, n)
        jobs = pl.ds(j0, n)
        xo, yo = tok_o[held].reshape(m, HALF), cot_o[held].reshape(m, HALF)
        pre_g = mm(xo, wg[own_cols, :])
        pre_u = mm(xo, wu[own_cols, :])
        d_h = mm_nt(yo, wd[:, own_cols])
        for d in range(n):
            pair(0, j0 + d).wait()
            pair(1, j0 + d).wait()
        xp, yp = tok_p[jobs].reshape(m, HALF), cot_p[jobs].reshape(m, HALF)
        pre_g += mm(xp, wg[oth_cols, :])
        pre_u += mm(xp, wu[oth_cols, :])
        d_h += mm_nt(yp, wd[:, oth_cols])
        sigma = jax.nn.sigmoid(pre_g)
        active = pre_g * sigma
        slope = sigma * (1.0 + pre_g * (1.0 - sigma))
        hid[ring] = (active * pre_u).astype(BF16).reshape(n, 128, FF)
        g = (d_h * pre_u * slope).astype(BF16)
        u = (d_h * active).astype(BF16)
        dg[ring] = g.reshape(n, 128, FF)
        du[ring] = u.reshape(n, 128, FF)
        back = mm_nt(g, wg[oth_cols, :]) + mm_nt(u, wu[oth_cols, :])
        theirs[ring] = back.astype(BF16).reshape(n, 128, HALF)
        for d in range(n):
            pair(2, j0 + d).start()
        back = mm_nt(g, wg[own_cols, :]) + mm_nt(u, wu[own_cols, :])
        mine[ring] = back.astype(BF16).reshape(n, 128, HALF)
        for d in range(n):
            for cp in keep(j0 + d):
                cp.start()

    def give_back(j):
        k = (j + 2) % RING
        pair(2, j).wait()
        s = (mine[k].astype(F32) + got[j].astype(F32)).astype(BF16)
        for n in range(4):
            rows = slice(n * 32, n * 32 + 32)
            stack = jnp.concatenate(
                [s[rows, p * 128 : (p + 1) * 128] for p in range(8)], axis=0
            )
            t0[k, n] = mm(mix[...], stack).astype(BF16).reshape(4, 4, 16, 128)
        launch(3, j)

    def collect(j):
        for n in range(4):
            rows = slice(n * 32, n * 32 + 32)
            v = mm(unmix[...], t3[j, n].reshape(256, 128)).astype(BF16)
            for p in range(8):
                rows_b[rows, p * 128 : (p + 1) * 128] = v[p * 32 : (p + 1) * 32]
        code = row_code(iota((1, 128), 1), j)
        pick = ind((code == subs[0, :, 0:1]) | (code == subs[1, :, 0:1])).astype(BF16)
        dn[...] += mm(pick, rows_b[...])

    def relay(stage):
        def fn(j):
            land(stage, j)
            launch(stage + 1, j)

        return fn

    def arrive(j):
        land(2, j)
        unpack(j)

    def finish(j):
        land(5, j)
        collect(j)

    def trio(group, fn):
        def one(c, carry):
            j = group * 3 - 2 + c
            pl.when((j >= 0) & (j < JOBS))(lambda: fn(j))
            return carry

        lax.fori_loop(0, 3, one, 0)

    def each(fn):
        def one(j, carry):
            fn(j)
            return carry

        lax.fori_loop(0, JOBS, one, 0)

    def step(g, carry):
        trio(g - 1, settle)
        pl.when(g == 0)(lambda: work(0, 1, pl.ds(2, 1)))
        pl.when((g > 0) & (g < 4))(lambda: work(3 * g - 2, 3, pl.ds(3 * (g % 2), 3)))
        trio(g - 2, relay(4))
        trio(g - 1, relay(3))
        trio(g + 1, arrive)
        trio(g - 3, finish)
        trio(g, give_back)
        return carry

    each(select)
    each(relay(0))
    each(relay(1))
    for cp in loads:
        cp.wait()
    arrive(0)
    lax.fori_loop(0, 7, step, 0)


def moe(mid, cot, gain, ids_t, prob, share, wg, wu, wd):
    return pl.pallas_call(
        moe_kernel,
        name="moe",
        out_shape=(
            jax.ShapeDtypeStruct((TOK, HALF), F32),
            jax.ShapeDtypeStruct((TOK, 128), F32),
            jax.ShapeDtypeStruct((ROWS, D), BF16),
            jax.ShapeDtypeStruct((ROWS, D), BF16),
            jax.ShapeDtypeStruct((ROWS, FF), BF16),
            jax.ShapeDtypeStruct((ROWS, FF), BF16),
            jax.ShapeDtypeStruct((ROWS, FF), BF16),
        ),
        in_specs=[VM] * 6 + [ANY] * 3,
        out_specs=(VM, VM, ANY, ANY, ANY, ANY, ANY),
        scratch_shapes=[
            pltpu.VMEM((TOK, 128), F32),
            pltpu.VMEM((TOK, 128), F32),
            pltpu.VMEM((TOK, HALF), BF16),
            pltpu.VMEM((8, TOK), jnp.int32),
            pltpu.VMEM((2, TOK, 128), jnp.int32),
            pltpu.VMEM((8, TOK), F32),
            pltpu.VMEM((256, 256), BF16),
            pltpu.VMEM((256, 256), BF16),
            pltpu.VMEM((JOBS, 4, 4, 4, 16, 256), BF16),
            pltpu.VMEM((JOBS, 4, 4, 4, 16, 256), BF16),
            pltpu.VMEM((JOBS, 4, 4, 4, 16, 256), BF16),
            pltpu.VMEM((JOBS, 4, 4, 4, 16, 256), BF16),
            pltpu.VMEM((6, 128, HALF), BF16),
            pltpu.VMEM((6, 128, HALF), BF16),
            pltpu.VMEM((JOBS, 128, HALF), BF16),
            pltpu.VMEM((JOBS, 128, HALF), BF16),
            pltpu.VMEM((RING, 128, FF), BF16),
            pltpu.VMEM((RING, 128, FF), BF16),
            pltpu.VMEM((RING, 128, FF), BF16),
            pltpu.VMEM((RING, 128, HALF), BF16),
            pltpu.VMEM((RING, 128, HALF), BF16),
            pltpu.VMEM((JOBS, 128, HALF), BF16),
            pltpu.VMEM((RING, 4, 4, 4, 16, 128), BF16),
            pltpu.VMEM((JOBS, 4, 4, 4, 16, 128), BF16),
            pltpu.VMEM((JOBS, 4, 4, 4, 16, 128), BF16),
            pltpu.VMEM((JOBS, 4, 4, 4, 16, 128), BF16),
            pltpu.VMEM((128, HALF), BF16),
            pltpu.VMEM((D, FF), BF16),
            pltpu.VMEM((D, FF), BF16),
            pltpu.VMEM((FF, D), BF16),
            pltpu.SemaphoreType.DMA((2,)),
            pltpu.SemaphoreType.DMA((6, JOBS, 3)),
            pltpu.SemaphoreType.DMA((6, JOBS, 3)),
            pltpu.SemaphoreType.DMA((6, JOBS)),
            pltpu.SemaphoreType.DMA((3, RING)),
            pltpu.SemaphoreType.DMA((3, JOBS)),
            pltpu.SemaphoreType.DMA((7, RING)),
            pltpu.SemaphoreType.DMA((3,)),
        ],
        compiler_params=pltpu.CompilerParams(
            collective_id=1, has_side_effects=True, vmem_limit_bytes=62 * 2**20
        ),
        cost_estimate=pl.CostEstimate(
            flops=20 * 10**9, bytes_accessed=30 * 10**6, transcendentals=655360
        ),
    )(mid, cot, gain, ids_t, prob, share, wg, wu, wd)


def tail_kernel(
    dn,
    mid,
    cot,
    gain,
    inv_in,
    bg,
    co,
    cgain,
    ow,
    gow,
    mgrad,
    gb,
    dco,
    in_mine,
    in_other,
    mg,
    send,
    recv,
):
    sp, tp = lax.axis_index("sp"), lax.axis_index("tp")
    other = (sp, 1 - tp)
    own_rows = pl.ds(pl.multiple_of(tp * HALF, HALF), HALF)
    oth_rows = pl.ds(pl.multiple_of((1 - tp) * HALF, HALF), HALF)
    greet(other)
    g_dn = dn[...] * gain[...].astype(F32).reshape(1, HALF)
    m32 = mid[...].astype(F32)
    inner = jnp.sum(m32 * g_dn, axis=1, keepdims=True)
    in_mine[...] = jnp.broadcast_to(inner, (TOK, 128))
    copy = pltpu.make_async_remote_copy(
        in_mine, in_other, send.at[0], recv.at[0], device_id=other, device_id_type=MESH
    )
    copy.start()
    b32 = bg[...].astype(F32)
    y32 = co[...].astype(F32)
    cg = cgain[...].astype(F32).reshape(1, 512)
    gated = b32 * y32
    same = ind(iota((512, 512), 0) // GROUP == iota((512, 512), 1) // GROUP)

    def group_mean(v):
        hi = v.astype(BF16)
        rest = v - hi.astype(F32)
        md = rest.astype(BF16)
        lo = (rest - md.astype(F32)).astype(BF16)
        ones = same.astype(BF16)
        return (mm(hi, ones) + mm(md, ones) + mm(lo, ones)) / GROUP

    rms = lax.rsqrt(group_mean(gated * gated) + epsilon)
    conv_normed = (gated * rms * cg).astype(BF16)
    copy.wait()
    inv = inv_in[:, 0:1]
    mean = (inner + in_other[:, 0:1]) / D
    total = cot[...].astype(F32) + inv * g_dn - m32 * (inv * inv * inv * mean)
    mgb = total.astype(BF16)
    mgrad[...] = mgb
    mg[tp] = mgb
    swap = pltpu.make_async_remote_copy(
        mg.at[tp], mg.at[tp], send.at[1], recv.at[1], device_id=other, device_id_type=MESH
    )
    swap.start()
    gow[own_rows, :] = mm_tn(mgb, conv_normed).astype(BF16)
    d_cn = mm(mgb, ow[own_rows, :])
    swap.wait()
    mo = mg[1 - tp]
    gow[oth_rows, :] = mm_tn(mo, conv_normed).astype(BF16)
    g_dc = cg * (d_cn + mm(mo, ow[oth_rows, :]))
    gmean = group_mean(gated * g_dc)
    d_gated = rms * g_dc - gated * (rms * rms * rms * gmean)
    gb[...] = (d_gated * y32).astype(BF16)
    dco[...] = d_gated * b32


def tail(*args):
    return pl.pallas_call(
        tail_kernel,
        name="tail",
        out_shape=(
            jax.ShapeDtypeStruct((D, 512), BF16),
            jax.ShapeDtypeStruct((TOK, HALF), BF16),
            jax.ShapeDtypeStruct((TOK, 512), BF16),
            jax.ShapeDtypeStruct((TOK, 512), F32),
        ),
        in_specs=[VM] * 9,
        out_specs=(VM,) * 4,
        scratch_shapes=[
            pltpu.VMEM((TOK, 128), F32),
            pltpu.VMEM((TOK, 128), F32),
            pltpu.VMEM((2, TOK, HALF), BF16),
            pltpu.SemaphoreType.DMA((2,)),
            pltpu.SemaphoreType.DMA((2,)),
        ],
        compiler_params=pltpu.CompilerParams(
            collective_id=2, has_side_effects=True, vmem_limit_bytes=62 * 2**20
        ),
        cost_estimate=pl.CostEstimate(
            flops=5 * 10**9, bytes_accessed=12 * 10**6, transcendentals=0
        ),
    )(*args)


def from_behind(block, axis, distance):
    devices = range(lax.axis_size(axis))
    route = [(i - distance, i) for i in devices if i - distance in devices]
    return lax.ppermute(block, axis, route)


def contract_rows(left, right):
    return lax.dot_general(
        left, right, (((0,), (0,)), ((), ())), preferred_element_type=jnp.float32
    )


def shards(
    mid_stream,
    layer_cot,
    ffn_gain,
    expert_ids,
    group_prob,
    first_share,
    expert_gate,
    expert_up,
    expert_down,
    out_weight,
    conv_gain,
    b_gate,
    c_gate,
    conv_in,
    conv_out,
    conv_taps,
):
    gain = ffn_gain
    d_normed, inv, tok, cot, hid, dg, du = moe(
        mid_stream,
        layer_cot,
        gain,
        expert_ids.T,
        group_prob,
        first_share,
        expert_gate[0],
        expert_up[0],
        expert_down[0],
    )
    grad_gate = contract_rows(tok, dg)[None]
    grad_up = contract_rows(tok, du)[None]
    grad_down = contract_rows(hid, cot)[None]
    gow, mid_grad, grad_b, d_conv_out = tail(
        d_normed,
        mid_stream,
        layer_cot,
        gain,
        inv,
        b_gate,
        conv_out,
        conv_gain,
        out_weight,
    )
    parts = lax.all_to_all(gow.reshape(NDEV, 32, 512), "sp", 0, 0, tiled=True)
    grad_out_weight = jnp.sum(parts.astype(jnp.float32), axis=0)
    following = from_behind(d_conv_out[:2], "sp", -1)
    extended = jnp.concatenate([d_conv_out, following], axis=0)
    taps = conv_taps.astype(jnp.float32)
    d_mixed = taps[2] * extended[:-2] + taps[1] * extended[1:-1] + taps[0] * extended[2:]
    grad_c = (d_mixed * conv_in.astype(jnp.float32)).astype(jnp.bfloat16)
    grad_conv_in = (d_mixed * c_gate.astype(jnp.float32)).astype(jnp.bfloat16)
    return (grad_gate, grad_up, grad_down, grad_out_weight, mid_grad, grad_b, grad_c, grad_conv_in)


def solution(mesh):
    placed = (
        P("sp", "tp"),
        P("sp", "tp"),
        P("tp"),
        P("sp", None),
        P("sp"),
        P("sp"),
        P("sp", None, "tp"),
        P("sp", None, "tp"),
        P("sp", "tp", None),
        P(None, "tp"),
        P("tp"),
        P("sp", "tp"),
        P("sp", "tp"),
        P("sp", "tp"),
        P("sp", "tp"),
        P(None, "tp"),
    )
    return jax.shard_map(
        shards,
        mesh=mesh,
        in_specs=placed,
        out_specs=(
            P("sp", None, "tp"),
            P("sp", None, "tp"),
            P("sp", "tp", None),
            P("sp", "tp"),
            P("sp", "tp"),
            P("sp", "tp"),
            P("sp", "tp"),
            P("sp", "tp"),
        ),
        check_vma=False,
    )
```

```python
import functools

import jax
import jax.numpy as jnp
from jax import lax
from jax.experimental import pallas as pl
from jax.experimental.pallas import tpu as pltpu
from jax.sharding import PartitionSpec as P

D = 2048
HALF = 1024
GROUP = 64
TOK = 320
FF = 512
NDEV = 64
ROWS = 1280
JOBS = 10
RING = 3
epsilon = 1e-06

F32 = jnp.float32
BF16 = jnp.bfloat16
MESH = pl.DeviceIdType.MESH
VM = pl.BlockSpec(memory_space=pltpu.VMEM)
ANY = pl.BlockSpec(memory_space=pl.ANY)


def mm(a, b):
    return jnp.dot(a, b, preferred_element_type=F32)


def mm_nt(a, b):
    return lax.dot_general(a, b, (((1,), (1,)), ((), ())), preferred_element_type=F32)


def mm_tn(a, b):
    return lax.dot_general(a, b, (((0,), (0,)), ((), ())), preferred_element_type=F32)


def iota(shape, dim):
    return lax.broadcasted_iota(jnp.int32, shape, dim)


def ind(mask):
    return jnp.where(mask, 1.0, 0.0)


def greet(other):
    barrier = pltpu.get_barrier_semaphore()
    pl.semaphore_signal(barrier, inc=1, device_id=other, device_id_type=MESH)
    pl.semaphore_wait(barrier, 1)


def lane_slots(ids, ids_t):
    earlier = iota((TOK, TOK), 0) < iota((TOK, TOK), 1)
    out = []
    for c in range(2):
        mine = ids_t[c : c + 1, :]
        same = ind(earlier & (ids[:, 0:1] == mine)) + ind(earlier & (ids[:, 1:2] == mine))
        rank = jnp.sum(same, axis=0, keepdims=True).astype(jnp.int32)
        out.append(mine * 32 + rank)
    return out


def row_slots(ids, ids_t):
    earlier = iota((TOK, TOK), 1) < iota((TOK, TOK), 0)
    out = []
    for c in range(2):
        mine = ids[:, c : c + 1]
        same = ind(earlier & (ids_t[0:1, :] == mine)) + ind(earlier & (ids_t[1:2, :] == mine))
        rank = jnp.sum(same, axis=1, keepdims=True).astype(jnp.int32)
        out.append(mine * 32 + rank)
    return out


def stride_of(dim):
    return (9 * dim * dim - 3 * dim + 2) // 2


def row_code(r, j):
    a, b, c = (stride_of((j + phase) % 3) for phase in range(3))
    e = ((r // 2) % 4) * c + ((r // 8) % 4) * b + (r // 32) * a
    return e * 32 + 2 * j + r % 2


def moe_kernel(
    mid,
    cot,
    gain,
    ids_t,
    prob,
    share,
    wg_in,
    wu_in,
    wd_in,
    bg,
    co,
    cgain,
    ow_in,
    gow_out,
    mgrad,
    gb,
    dco,
    tok_out,
    cot_out,
    hid_out,
    dg_out,
    du_out,
    sq_mine,
    sq_other,
    normed,
    lanes,
    subs,
    weights,
    mix,
    unmix,
    s0,
    r1,
    r2,
    r3,
    tok_o,
    cot_o,
    tok_p,
    cot_p,
    hid,
    dg,
    du,
    mine,
    theirs,
    got,
    t0,
    t1,
    t2,
    t3,
    rows_b,
    wg,
    wu,
    wd,
    sq_sem,
    send,
    recv,
    local,
    psend,
    precv,
    osem,
    wsem,
    dn,
    inv_out,
    in_other,
    rms_s,
    cn_s,
    tsend,
    trecv,
):
    sp, tp = lax.axis_index("sp"), lax.axis_index("tp")
    other = (sp, 1 - tp)
    own_cols = pl.ds(pl.multiple_of(tp * HALF, HALF), HALF)
    oth_cols = pl.ds(pl.multiple_of((1 - tp) * HALF, HALF), HALF)

    def place(dim):
        return (sp // stride_of(dim)) % 4

    def peer(dim, off):
        c = (place(dim) + off) % 4
        return c, (sp + (c - place(dim)) * stride_of(dim), tp)

    barrier = pltpu.get_barrier_semaphore()
    pl.semaphore_signal(barrier, inc=1, device_id=other, device_id_type=MESH)
    for dim in range(3):
        for off in (1, 2, 3):
            pl.semaphore_signal(barrier, inc=1, device_id=peer(dim, off)[1], device_id_type=MESH)
    loads = [
        pltpu.make_async_copy(a, b, wsem.at[n])
        for n, (a, b) in enumerate(((wg_in, wg), (wu_in, wu), (wd_in, wd)))
    ]
    for cp in loads:
        cp.start()
    m32 = mid[...].astype(F32)
    sq = jnp.sum(m32 * m32, axis=1, keepdims=True)
    sq_mine[...] = jnp.broadcast_to(sq, (TOK, 128))
    eye = ind(iota((TOK, TOK), 0) == iota((TOK, TOK), 1)).astype(BF16)
    ids = mm_nt(eye, ids_t[...].astype(F32).astype(BF16)).astype(jnp.int32)
    l0, l1 = lane_slots(ids, ids_t[...])
    lanes[0:1, :] = l0
    lanes[1:2, :] = l1
    p1 = prob[...].reshape(1, TOK)
    f1 = share[...].reshape(1, TOK)
    weights[0:1, :] = p1 * f1
    weights[1:2, :] = p1 * (1.0 - f1)
    i = iota((256, 256), 0)
    c = iota((256, 256), 1)
    mix[...] = ind(c == ((i // 2) % 8) * 32 + (i // 16) * 2 + i % 2).astype(BF16)
    dn[...] = jnp.zeros((TOK, HALF), F32)
    pl.semaphore_wait(barrier, 10)
    copy = pltpu.make_async_remote_copy(
        sq_mine, sq_other, sq_sem.at[0], sq_sem.at[1], device_id=other, device_id_type=MESH
    )
    copy.start()
    b0, b1 = row_slots(ids, ids_t[...])
    subs[0] = jnp.broadcast_to(b0, (TOK, 128))
    subs[1] = jnp.broadcast_to(b1, (TOK, 128))
    unmix[...] = ind(c == ((i // 2) % 16) * 16 + (i // 32) * 2 + i % 2).astype(BF16)
    copy.wait()
    inv = lax.rsqrt((sq + sq_other[:, 0:1]) / D + epsilon)
    inv_out[...] = jnp.broadcast_to(inv, (TOK, 128))
    normed[...] = (m32 * inv * gain[...].astype(F32).reshape(1, HALF)).astype(BF16)

    def part_at(buf, lead, depth, k):
        if depth == 0:
            return buf.at[lead, k]
        if depth == 1:
            return buf.at[lead, :, k]
        return buf.at[lead, :, :, k]

    def hop(stage, j):
        src, lead, dst = (
            (s0, j % 7, r1),
            (r1, j, r2),
            (r2, j, r3),
            (t0, (j + 2) % RING, t1),
            (t1, j, t2),
            (t2, j, t3),
        )[stage]
        dim = (j + (0, 1, 2, 2, 1, 0)[stage]) % 3
        depth = stage % 3
        me = place(dim)
        copies = []
        for off in (2, 1, 3):
            there, device = peer(dim, off)
            copies.append(
                pltpu.make_async_remote_copy(
                    part_at(src, lead, depth, there),
                    dst.at[j, me],
                    send.at[stage, j, off - 1],
                    recv.at[stage, j, off - 1],
                    device_id=device,
                    device_id_type=MESH,
                )
            )
        copies.append(
            pltpu.make_async_copy(
                part_at(src, lead, depth, me), dst.at[j, me], local.at[stage, j]
            )
        )
        return copies

    def launch(stage, j):
        for cp in hop(stage, j):
            cp.start()

    def land(stage, j):
        for cp in hop(stage, j):
            cp.wait()

    def pair(kind, j):
        src, dst = (
            (tok_o.at[(j + 2) % 6], tok_p.at[j]),
            (cot_o.at[(j + 2) % 6], cot_p.at[j]),
            (theirs.at[(j + 2) % RING], got.at[(j + 2) % 6]),
        )[kind]
        return pltpu.make_async_remote_copy(
            src,
            dst,
            psend.at[kind, j % RING],
            precv.at[kind, j],
            device_id=other,
            device_id_type=MESH,
        )

    def keep(j):
        rows = pl.ds(pl.multiple_of(j * 128, 128), 128)
        k = (j + 2) % RING
        pairs = (
            (tok_o.at[(j + 2) % 6], tok_out.at[rows, own_cols]),
            (tok_p.at[j], tok_out.at[rows, oth_cols]),
            (cot_o.at[(j + 2) % 6], cot_out.at[rows, own_cols]),
            (cot_p.at[j], cot_out.at[rows, oth_cols]),
            (hid.at[k], hid_out.at[rows]),
            (dg.at[k], dg_out.at[rows]),
            (du.at[k], du_out.at[rows]),
        )
        return [pltpu.make_async_copy(a, b, osem.at[n, j % RING]) for n, (a, b) in enumerate(pairs)]

    def select(j):
        r = iota((128, 1), 0)
        code = row_code(r, j)
        hit0 = code == lanes[0:1, :]
        hit1 = code == lanes[1:2, :]
        pick = ind(hit0 | hit1).astype(BF16)
        weight = jnp.sum(
            jnp.where(hit0, weights[0:1, :], 0.0) + jnp.where(hit1, weights[1:2, :], 0.0),
            axis=1,
            keepdims=True,
        )
        a = mm(pick, normed[...]).astype(BF16)
        b = (mm(pick, cot[...]) * weight).astype(BF16)
        for n in range(4):
            rows = slice(n * 32, n * 32 + 32)
            stack = jnp.concatenate(
                [v[rows, p * 256 : (p + 1) * 256] for v in (a, b) for p in range(4)], axis=0
            )
            s0[j % 7, n] = mm(mix[...], stack).astype(BF16).reshape(4, 4, 16, 256)
        launch(0, j)

    def settle(j):
        for cp in keep(j):
            cp.wait()

    def unpack(j):
        k = (j + 2) % 6
        for n in range(4):
            rows = slice(n * 32, n * 32 + 32)
            v = mm(unmix[...], r3[j, n].reshape(256, 256)).astype(BF16)
            for p in range(4):
                cols = slice(p * 256, (p + 1) * 256)
                tok_o[k, rows, cols] = v[p * 32 : (p + 1) * 32]
                cot_o[k, rows, cols] = v[128 + p * 32 : 128 + (p + 1) * 32]
        pair(0, j).start()
        pair(1, j).start()

    def back_rows(buf, ring, g, u, half, n):
        for h in range(2):
            w = pl.ds(pl.multiple_of(half * HALF + h * 512, 512), 512)
            back = mm_nt(g, wg[w, :]) + mm_nt(u, wu[w, :])
            buf[ring, :, h * 512 : (h + 1) * 512] = back.astype(BF16).reshape(n, 128, 512)

    def work(j0, n, held):
        m = n * 128
        ring = pl.ds(2 if n == 1 else 0, n)
        jobs = pl.ds(j0, n)
        xo, yo = tok_o[held].reshape(m, HALF), cot_o[held].reshape(m, HALF)
        pre_g = mm(xo, wg[own_cols, :])
        pre_u = mm(xo, wu[own_cols, :])
        d_h = mm_nt(yo, wd[:, own_cols])
        for d in range(n):
            pair(0, j0 + d).wait()
            pair(1, j0 + d).wait()
        xp, yp = tok_p[jobs].reshape(m, HALF), cot_p[jobs].reshape(m, HALF)
        pre_g += mm(xp, wg[oth_cols, :])
        pre_u += mm(xp, wu[oth_cols, :])
        d_h += mm_nt(yp, wd[:, oth_cols])
        sigma = jax.nn.sigmoid(pre_g)
        active = pre_g * sigma
        slope = sigma * (1.0 + pre_g * (1.0 - sigma))
        hid[ring] = (active * pre_u).astype(BF16).reshape(n, 128, FF)
        g = (d_h * pre_u * slope).astype(BF16)
        u = (d_h * active).astype(BF16)
        dg[ring] = g.reshape(n, 128, FF)
        du[ring] = u.reshape(n, 128, FF)
        back_rows(theirs, ring, g, u, 1 - tp, n)
        for d in range(n):
            pair(2, j0 + d).start()
        back_rows(mine, ring, g, u, tp, n)
        for d in range(n):
            for cp in keep(j0 + d):
                cp.start()

    def give_back(j):
        k = (j + 2) % RING
        pair(2, j).wait()
        s = (mine[k].astype(F32) + got[(j + 2) % 6].astype(F32)).astype(BF16)
        for n in range(4):
            rows = slice(n * 32, n * 32 + 32)
            stack = jnp.concatenate(
                [s[rows, p * 128 : (p + 1) * 128] for p in range(8)], axis=0
            )
            t0[k, n] = mm(mix[...], stack).astype(BF16).reshape(4, 4, 16, 128)
        launch(3, j)

    def collect(j):
        for n in range(4):
            rows = slice(n * 32, n * 32 + 32)
            v = mm(unmix[...], t3[j, n].reshape(256, 128)).astype(BF16)
            for p in range(8):
                rows_b[rows, p * 128 : (p + 1) * 128] = v[p * 32 : (p + 1) * 32]
        code = row_code(iota((1, 128), 1), j)
        pick = ind((code == subs[0, :, 0:1]) | (code == subs[1, :, 0:1])).astype(BF16)
        dn[...] += mm(pick, rows_b[...])

    def relay(stage):
        def fn(j):
            land(stage, j)
            launch(stage + 1, j)

        return fn

    def arrive(j):
        land(2, j)
        unpack(j)

    def finish(j):
        land(5, j)
        collect(j)

    def trio(group, fn):
        def one(c, carry):
            j = group * 3 - 2 + c
            pl.when((j >= 0) & (j < JOBS))(lambda: fn(j))
            return carry

        lax.fori_loop(0, 3, one, 0)

    def each(fn, lo, hi):
        def one(j, carry):
            fn(j)
            return carry

        lax.fori_loop(lo, hi, one, 0)

    weigh = pltpu.make_async_copy(ow_in, wu, wsem.at[0])

    def group_mean(v):
        hi = v.astype(BF16)
        rest = v - hi.astype(F32)
        md = rest.astype(BF16)
        lo = (rest - md.astype(F32)).astype(BF16)
        ones = ind(iota((512, 512), 0) // GROUP == iota((512, 512), 1) // GROUP).astype(BF16)
        return (mm(hi, ones) + mm(md, ones) + mm(lo, ones)) / GROUP

    def conv_stats():
        gated = bg[...].astype(F32) * co[...].astype(F32)
        rms = lax.rsqrt(group_mean(gated * gated) + epsilon)
        rms_s[...] = rms
        cn_s[...] = (gated * rms * cgain[...].astype(F32).reshape(1, 512)).astype(BF16)

    def catch_up():
        each(relay(1), 4, 7)
        trio(1, give_back)
        each(relay(1), 7, JOBS)

    def step(g, carry):
        trio(g - 1, settle)
        pl.when(g == 0)(lambda: work(0, 1, pl.ds(2, 1)))
        pl.when((g > 0) & (g < 4))(lambda: work(3 * g - 2, 3, pl.ds(3 * (g % 2), 3)))
        trio(g - 2, relay(4))
        trio(g - 1, relay(3))
        pl.when(g == 1)(catch_up)
        trio(g + 1, arrive)
        trio(g - 3, finish)
        pl.when(g == 4)(lambda: weigh.start())
        pl.when(g == 5)(conv_stats)
        pl.when(g != 1)(lambda: trio(g, give_back))
        return carry

    each(select, 0, 7)
    each(relay(0), 0, 4)
    each(select, 7, JOBS)
    each(relay(1), 0, 4)
    each(relay(0), 4, JOBS)
    for cp in loads:
        cp.wait()
    arrive(0)
    lax.fori_loop(0, 7, step, 0)
    g_dn = dn[...] * gain[...].astype(F32).reshape(1, HALF)
    m32 = mid[...].astype(F32)
    inner = jnp.sum(m32 * g_dn, axis=1, keepdims=True)
    sq_mine[...] = jnp.broadcast_to(inner, (TOK, 128))
    copy = pltpu.make_async_remote_copy(
        sq_mine, in_other, tsend.at[0], trecv.at[0], device_id=other, device_id_type=MESH
    )
    copy.start()
    weigh.wait()
    inv = inv_out[:, 0:1]
    copy.wait()
    mean = (inner + in_other[:, 0:1]) / D
    total = cot[...].astype(F32) + inv * g_dn - m32 * (inv * inv * inv * mean)
    mgb = total.astype(BF16)
    mgrad[...] = mgb
    swap = pltpu.make_async_remote_copy(
        mgrad, normed, tsend.at[1], trecv.at[1], device_id=other, device_id_type=MESH
    )
    swap.start()
    cn = cn_s[...]
    wg[own_cols, :] = mm_tn(mgb, cn).astype(BF16)
    d_cn = mm(mgb, wu[own_cols, :])
    b32 = bg[...].astype(F32)
    y32 = co[...].astype(F32)
    gated = b32 * y32
    rms = rms_s[...]
    swap.wait()
    mo = normed[...]
    wg[oth_cols, :] = mm_tn(mo, cn).astype(BF16)
    leave = pltpu.make_async_copy(wg, gow_out, wsem.at[1])
    leave.start()
    g_dc = cgain[...].astype(F32).reshape(1, 512) * (d_cn + mm(mo, wu[oth_cols, :]))
    gmean = group_mean(gated * g_dc)
    d_gated = rms * g_dc - gated * (rms * rms * rms * gmean)
    gb[...] = (d_gated * y32).astype(BF16)
    dco[...] = d_gated * b32
    leave.wait()


def moe(*args):
    return pl.pallas_call(
        moe_kernel,
        name="moe",
        out_shape=(
            jax.ShapeDtypeStruct((D, 512), BF16),
            jax.ShapeDtypeStruct((TOK, HALF), BF16),
            jax.ShapeDtypeStruct((TOK, 512), BF16),
            jax.ShapeDtypeStruct((TOK, 512), F32),
            jax.ShapeDtypeStruct((ROWS, D), BF16),
            jax.ShapeDtypeStruct((ROWS, D), BF16),
            jax.ShapeDtypeStruct((ROWS, FF), BF16),
            jax.ShapeDtypeStruct((ROWS, FF), BF16),
            jax.ShapeDtypeStruct((ROWS, FF), BF16),
        ),
        in_specs=[VM] * 6 + [ANY] * 3 + [VM] * 3 + [ANY],
        out_specs=(ANY, VM, VM, VM, ANY, ANY, ANY, ANY, ANY),
        scratch_shapes=[
            pltpu.VMEM((TOK, 128), F32),
            pltpu.VMEM((TOK, 128), F32),
            pltpu.VMEM((TOK, HALF), BF16),
            pltpu.VMEM((8, TOK), jnp.int32),
            pltpu.VMEM((2, TOK, 128), jnp.int32),
            pltpu.VMEM((8, TOK), F32),
            pltpu.VMEM((256, 256), BF16),
            pltpu.VMEM((256, 256), BF16),
            pltpu.VMEM((7, 4, 4, 4, 16, 256), BF16),
            pltpu.VMEM((JOBS, 4, 4, 4, 16, 256), BF16),
            pltpu.VMEM((JOBS, 4, 4, 4, 16, 256), BF16),
            pltpu.VMEM((JOBS, 4, 4, 4, 16, 256), BF16),
            pltpu.VMEM((6, 128, HALF), BF16),
            pltpu.VMEM((6, 128, HALF), BF16),
            pltpu.VMEM((JOBS, 128, HALF), BF16),
            pltpu.VMEM((JOBS, 128, HALF), BF16),
            pltpu.VMEM((RING, 128, FF), BF16),
            pltpu.VMEM((RING, 128, FF), BF16),
            pltpu.VMEM((RING, 128, FF), BF16),
            pltpu.VMEM((RING, 128, HALF), BF16),
            pltpu.VMEM((RING, 128, HALF), BF16),
            pltpu.VMEM((6, 128, HALF), BF16),
            pltpu.VMEM((RING, 4, 4, 4, 16, 128), BF16),
            pltpu.VMEM((JOBS, 4, 4, 4, 16, 128), BF16),
            pltpu.VMEM((JOBS, 4, 4, 4, 16, 128), BF16),
            pltpu.VMEM((JOBS, 4, 4, 4, 16, 128), BF16),
            pltpu.VMEM((128, HALF), BF16),
            pltpu.VMEM((D, FF), BF16),
            pltpu.VMEM((D, FF), BF16),
            pltpu.VMEM((FF, D), BF16),
            pltpu.SemaphoreType.DMA((2,)),
            pltpu.SemaphoreType.DMA((6, JOBS, 3)),
            pltpu.SemaphoreType.DMA((6, JOBS, 3)),
            pltpu.SemaphoreType.DMA((6, JOBS)),
            pltpu.SemaphoreType.DMA((3, RING)),
            pltpu.SemaphoreType.DMA((3, JOBS)),
            pltpu.SemaphoreType.DMA((7, RING)),
            pltpu.SemaphoreType.DMA((3,)),
            pltpu.VMEM((TOK, HALF), F32),
            pltpu.VMEM((TOK, 128), F32),
            pltpu.VMEM((TOK, 128), F32),
            pltpu.VMEM((TOK, 512), F32),
            pltpu.VMEM((TOK, 512), BF16),
            pltpu.SemaphoreType.DMA((2,)),
            pltpu.SemaphoreType.DMA((2,)),
        ],
        compiler_params=pltpu.CompilerParams(
            collective_id=1, has_side_effects=True, vmem_limit_bytes=67043328
        ),
        cost_estimate=pl.CostEstimate(
            flops=20 * 10**9, bytes_accessed=30 * 10**6, transcendentals=655360
        ),
    )(*args)


def from_behind(block, axis, distance):
    devices = range(lax.axis_size(axis))
    route = [(i - distance, i) for i in devices if i - distance in devices]
    return lax.ppermute(block, axis, route)


def contract_rows(left, right):
    return lax.dot_general(
        left, right, (((0,), (0,)), ((), ())), preferred_element_type=jnp.float32
    )


def shards(
    mid_stream,
    layer_cot,
    ffn_gain,
    expert_ids,
    group_prob,
    first_share,
    expert_gate,
    expert_up,
    expert_down,
    out_weight,
    conv_gain,
    b_gate,
    c_gate,
    conv_in,
    conv_out,
    conv_taps,
):
    gow, mid_grad, grad_b, d_conv_out, tok, cot, hid, dg, du = moe(
        mid_stream,
        layer_cot,
        ffn_gain,
        expert_ids.T,
        group_prob,
        first_share,
        expert_gate[0],
        expert_up[0],
        expert_down[0],
        b_gate,
        conv_out,
        conv_gain,
        out_weight,
    )
    grad_gate = contract_rows(tok, dg)[None]
    grad_up = contract_rows(tok, du)[None]
    grad_down = contract_rows(hid, cot)[None]
    parts = lax.all_to_all(gow.reshape(NDEV, 32, 512), "sp", 0, 0, tiled=True)
    grad_out_weight = jnp.sum(parts.astype(jnp.float32), axis=0)
    following = from_behind(d_conv_out[:2], "sp", -1)
    extended = jnp.concatenate([d_conv_out, following], axis=0)
    taps = conv_taps.astype(jnp.float32)
    d_mixed = taps[2] * extended[:-2] + taps[1] * extended[1:-1] + taps[0] * extended[2:]
    grad_c = (d_mixed * conv_in.astype(jnp.float32)).astype(jnp.bfloat16)
    grad_conv_in = (d_mixed * c_gate.astype(jnp.float32)).astype(jnp.bfloat16)
    return (grad_gate, grad_up, grad_down, grad_out_weight, mid_grad, grad_b, grad_c, grad_conv_in)


def solution(mesh):
    placed = (
        P("sp", "tp"),
        P("sp", "tp"),
        P("tp"),
        P("sp", None),
        P("sp"),
        P("sp"),
        P("sp", None, "tp"),
        P("sp", None, "tp"),
        P("sp", "tp", None),
        P(None, "tp"),
        P("tp"),
        P("sp", "tp"),
        P("sp", "tp"),
        P("sp", "tp"),
        P("sp", "tp"),
        P(None, "tp"),
    )
    return jax.shard_map(
        shards,
        mesh=mesh,
        in_specs=placed,
        out_specs=(
            P("sp", None, "tp"),
            P("sp", None, "tp"),
            P("sp", "tp", None),
            P("sp", "tp"),
            P("sp", "tp"),
            P("sp", "tp"),
            P("sp", "tp"),
            P("sp", "tp"),
        ),
        check_vma=False,
    )
```
